256 devices in a mesh: ep: 32 (over z, x), tp: 8 (over y, core).
Axes of the slice: x: 4, y: 4, z: 8, core: 2. Of those that a mesh axis runs over, the one named last changes fastest.
Arguments:
- tokens: bfloat16 [512, 2048], P('ep'), may hold values from -6 to 6
- norm_attn: float32 [2048], replicated, may hold values from 0.1 to 1.9
- w_query: bfloat16 [2048, 1024], P(None, 'tp'), may hold values from -0.125 to 0.125
- w_key: bfloat16 [2048, 1024], P(None, 'tp'), may hold values from -0.125 to 0.125
- w_value: bfloat16 [2048, 1024], P(None, 'tp'), may hold values from -0.125 to 0.125
- w_forget: bfloat16 [2048, 16], P(None, 'tp'), may hold values from -0.125 to 0.125
- forget_bias: float32 [16], P('tp'), may hold values from -1.5 to 1.5
- w_output: bfloat16 [1024, 2048], P('tp'), may hold values from -0.1875 to 0.1875
- key_cache: bfloat16 [512, 1024, 1024], P('ep', None, 'tp'), may hold values from -488 to 488
- value_cache: bfloat16 [512, 1024, 1024], P('ep', None, 'tp'), may hold values from -6 to 6
- gate_cache: float32 [512, 16, 1024], P('ep', 'tp'), may hold values from -132 to 0, as said below
- lengths: int32 [512], P('ep'), may hold values from 256 to 1024
- norm_ffn: float32 [2048], replicated, may hold values from 0.1 to 1.9
- route_group: int32 [512], P('ep'), may hold values from 0 to 3
- route_slot: int32 [512, 2], P('ep'), may hold values from 0 to 7, as said below
- route_weight: float32 [512, 2], P('ep'), may hold values from 0.2 to 1
- expert_gate: bfloat16 [32, 2048, 1024], P('ep', None, 'tp'), may hold values from -0.125 to 0.125
- expert_up: bfloat16 [32, 2048, 1024], P('ep', None, 'tp'), may hold values from -0.125 to 0.125
- expert_down: bfloat16 [32, 1024, 2048], P('ep', 'tp'), may hold values from -0.1875 to 0.1875
- dense_gate: bfloat16 [2048, 4096], P('tp', 'ep'), may hold values from -0.125 to 0.125
- dense_up: bfloat16 [2048, 4096], P('tp', 'ep'), may hold values from -0.125 to 0.125
- dense_down: bfloat16 [4096, 2048], P('ep', 'tp'), may hold values from -0.09375 to 0.09375
- mix_vector: float32 [2048], replicated, may hold values from -0.125 to 0.125
Outputs:
- mixed_out: bfloat16 [512, 2048], P('ep', 'tp')
The draws below stay inside these ranges and needn't reach their ends.
Inputs may be any that keep to these rules, and one draw needn't show every extreme that they name: `route_slot`: the two picks of a token are different experts of its group. Among the sequences of one index of ep at most 2 picks name one expert, and in every draw some expert gets exactly 2 picks from every index of ep. `gate_cache`: along the positions of each sequence and head the values never rise.
All inputs are finite; a program needn't handle non-finite values.
Results may differ from the reference program's by a relative error of at most 0.014.
Values may be sent and summed in bfloat16 or wider, within the bound.
No kernel may reach another device: no remote copies, remote signals or barrier semaphores. Data moves between devices by JAX's collectives and lax.ppermute only.
A program may use at most 64 MiB of HBM per device.

```python
import jax
import jax.numpy as jnp
import numpy as np
from jax import lax

D = 2048
HEADS = 16
HEAD_DIM = 64
GROUPS = 4
EXPERTS_PER_GROUP = 8
EXPERT_FF = 1024
DENSE_FF = 4096
TOP_K = 2
SEQ_DEV = 16
STORED_ENTRIES = 1024
EXPERTS = 32
STREAM_COUNT = 512
N_TP = 8


def routing_table(key):
    block_count = STREAM_COUNT // SEQ_DEV
    quarter = SEQ_DEV // 4
    eighth = SEQ_DEV // 8
    group_sizes = [SEQ_DEV // 2, quarter, eighth, SEQ_DEV - SEQ_DEV // 2 - quarter - eighth]
    member = np.concatenate([np.full(size_now, order_now) for order_now, size_now in enumerate(group_sizes)]).astype(np.int32)
    within = np.concatenate([np.arange(size_now) for size_now in group_sizes]).astype(np.int32)
    hot_order = jax.random.permutation(jax.random.fold_in(key, 11), GROUPS)

    def one_block(block_index):
        block_key = jax.random.fold_in(jax.random.fold_in(key, 12), block_index)
        derived_seeds = jax.random.split(block_key, 4)
        rest_order = jax.random.permutation(derived_seeds[0], GROUPS - 1)
        own_order = jnp.concatenate([hot_order[:1], hot_order[1:][rest_order]])
        is_hot = jax.random.randint(derived_seeds[1], (), 0, 2)
        group_order = jnp.where(is_hot == 1, hot_order, own_order)
        expert_orders = jax.vmap(lambda one_key: jax.random.permutation(one_key, EXPERTS_PER_GROUP))(jax.random.split(derived_seeds[2], GROUPS))
        groups = group_order[member]
        first_slot = expert_orders[member, within % EXPERTS_PER_GROUP]
        second = expert_orders[member, (within + 1) % EXPERTS_PER_GROUP]
        shuffle = jax.random.permutation(derived_seeds[3], SEQ_DEV)
        return (groups[shuffle], jnp.stack([first_slot, second], axis=1)[shuffle])
    groups, slots = jax.vmap(one_block)(jnp.arange(block_count))
    return (groups.reshape(-1).astype(jnp.int32), slots.reshape(-1, 2).astype(jnp.int32))


def draw_route_group(key, part):
    return routing_table(jax.random.fold_in(key, 5))[0]


def draw_route_slot(key, part):
    return routing_table(jax.random.fold_in(key, 5))[1]


def draw_gate_cache(key, part):
    derived_seeds = jax.random.split(key, 5)
    lagging_marker = jax.random.randint(derived_seeds[0], (HEADS,), 0, 2).astype(jnp.float32)
    step_rate = lagging_marker * (1.0 / STORED_ENTRIES) + (1.0 - lagging_marker) * (1.0 / 40.0)
    seq_scale = jnp.exp(jax.random.uniform(derived_seeds[1], (STREAM_COUNT, 1, 1), jnp.float32, -0.7, 0.7))
    roughness = jnp.exp(jax.random.uniform(derived_seeds[2], (STREAM_COUNT, HEADS, STORED_ENTRIES), jnp.float32, -0.7, 0.7))
    recorded_moments = -step_rate[None, :, None] * seq_scale * roughness
    run_opening = jax.random.randint(derived_seeds[3], (STREAM_COUNT, 3), 0, STORED_ENTRIES)
    entry_indices = jnp.arange(STORED_ENTRIES)
    run_extents = jnp.any(entry_indices[None, None, :] == run_opening[:, :, None], axis=1).astype(jnp.float32)
    run_extent = jnp.log(jax.random.uniform(derived_seeds[4], (STREAM_COUNT, 1, STORED_ENTRIES), jnp.float32, 0.5, 0.8))
    recorded_moments = recorded_moments + run_extents[:, None, :] * lagging_marker[None, :, None] * run_extent
    return jnp.cumsum(recorded_moments, axis=-1)


def draw_key_cache(key, part):
    derived_seeds = jax.random.split(key, 1)
    width_all = HEADS * HEAD_DIM
    base = jnp.clip(jax.random.normal(derived_seeds[0], (STREAM_COUNT, STORED_ENTRIES, width_all), jnp.float32), -4.0, 4.0)
    return base.astype(jnp.bfloat16)


def touch_ends(values, own_key, smallest, largest):
    longest = values.shape.index(max(values.shape))
    spots = []
    for shift in (0, 1):
        where = [jax.random.randint(jax.random.fold_in(own_key, axis), (), 0, length) for axis, length in enumerate(values.shape)]
        where[longest] = (where[longest] + shift) % values.shape[longest]
        spots.append(tuple(where))
    return values.at[spots[0]].set(smallest).at[spots[1]].set(largest)


def level_of(key, shape, cuts, least, top_value):
    def one(axis_at, shards_of):
        steps = jax.random.uniform(jax.random.fold_in(jax.random.fold_in(key, 6), axis_at), (shards_of,), jnp.float32, least / len(cuts), top_value / len(cuts))
        return jnp.repeat(jnp.exp(steps), shape[axis_at] // shards_of).reshape((-1,) + (1,) * (len(shape) - axis_at - 1))

    gain = one(*cuts[0])
    for cut in cuts[1:]:
        gain = gain * one(*cut)
    return gain


def centred(stream_key, extent, scale, reach, cuts=(), held_as=jnp.bfloat16):
    entries = jax.random.normal(stream_key, extent, jnp.float32) * scale
    if len(cuts) > 0:
        entries = level_of(stream_key, extent, cuts, -0.22, 0.18) * entries
    return jnp.clip(entries, min=-reach, max=reach).astype(held_as)


def setup_inputs(seed: int = 0) -> dict:
    splits = jax.random.split(jax.random.key(seed), 24)
    return {
        "tokens": centred(splits[0], (STREAM_COUNT, D), 1.0, 6.0, ((0, 32),)),
        "norm_attn": jnp.clip(1.0 + 0.18 * jax.random.normal(splits[1], (D,), jnp.float32), 0.1, 1.9),
        "w_query": centred(splits[2], (D, HEADS * HEAD_DIM), D ** -0.5, 0.125, ((1, 8),)),
        "w_key": centred(splits[3], (D, HEADS * HEAD_DIM), D ** -0.5, 0.125, ((1, 8),)),
        "w_value": centred(splits[4], (D, HEADS * HEAD_DIM), D ** -0.5, 0.125, ((1, 8),)),
        "w_forget": centred(splits[5], (D, HEADS), D ** -0.5, 0.125, ((1, 8),)),
        "forget_bias": jnp.clip(jax.random.uniform(splits[6], (HEADS,), jnp.float32, -1.5, 1.5) * level_of(splits[6], (HEADS,), ((0, 8),), -0.4, 0.0), -1.5, 1.5),
        "w_output": centred(splits[7], (HEADS * HEAD_DIM, D), (HEADS * HEAD_DIM) ** -0.5, 0.1875, ((0, 8),)),
        "key_cache": draw_key_cache(jax.random.fold_in(splits[23], 71), 0),
        "value_cache": centred(splits[9], (STREAM_COUNT, STORED_ENTRIES, HEADS * HEAD_DIM), 1.0, 6.0, ((0, 32), (2, 8))),
        "gate_cache": draw_gate_cache(jax.random.fold_in(splits[23], 71), 0),
        "lengths": touch_ends(jax.random.randint(splits[11], (STREAM_COUNT,), STORED_ENTRIES // 4, STORED_ENTRIES + 1), jax.random.fold_in(splits[11], 1), STORED_ENTRIES // 4, STORED_ENTRIES).astype(jnp.int32),
        "norm_ffn": jnp.clip(1.0 + 0.18 * jax.random.normal(splits[12], (D,), jnp.float32), 0.1, 1.9),
        "route_group": draw_route_group(jax.random.fold_in(splits[23], 71), 0),
        "route_slot": draw_route_slot(jax.random.fold_in(splits[23], 71), 0),
        "route_weight": jnp.clip(0.2 + 0.8 * jax.random.uniform(splits[15], (STREAM_COUNT, TOP_K), jnp.float32) ** level_of(splits[15], (STREAM_COUNT, TOP_K), ((0, 32),), -0.2, 0.2), 0.2, 1.0),
        "expert_gate": centred(splits[16], (EXPERTS, D, EXPERT_FF), D ** -0.5, 0.125, ((0, 32), (2, 8))),
        "expert_up": centred(splits[17], (EXPERTS, D, EXPERT_FF), D ** -0.5, 0.125, ((0, 32), (2, 8))),
        "expert_down": centred(splits[18], (EXPERTS, EXPERT_FF, D), EXPERT_FF ** -0.5, 0.1875, ((0, 32), (1, 8))),
        "dense_gate": centred(splits[19], (D, DENSE_FF), D ** -0.5, 0.125, ((0, 8), (1, 32))),
        "dense_up": centred(splits[20], (D, DENSE_FF), D ** -0.5, 0.125, ((0, 8), (1, 32))),
        "dense_down": centred(splits[21], (DENSE_FF, D), DENSE_FF ** -0.5, 0.09375, ((0, 32), (1, 8))),
        "mix_vector": centred(splits[22], (D,), D ** -0.5, 0.125, (), jnp.float32),
    }


EPS = 1e-06

def rms_scale(row_block, gain_vector):
    row_block = row_block.astype(jnp.float32)
    return row_block * lax.rsqrt(lax.optimization_barrier(jnp.mean(row_block * row_block, axis=-1, keepdims=True)) + EPS) * gain_vector

def bf16_round(array):
    return lax.optimization_barrier(array.astype(jnp.bfloat16)).astype(jnp.float32)

def attend_one(packed):
    queries, key_new, value_new, forget_log, key_rows, value_rows, gate_row, length = packed
    heads = gate_row.shape[0]
    cache_len = gate_row.shape[1]
    head_size = queries.shape[0] // heads
    score_scale = head_size ** (-0.5)
    query_h = queries.astype(jnp.float32).reshape(heads, head_size)
    key_h = key_rows.astype(jnp.float32).reshape(cache_len, heads, head_size)
    value_h = value_rows.astype(jnp.float32).reshape(cache_len, heads, head_size)
    entry_indices = jnp.arange(cache_len, dtype=jnp.int32)
    last_gate = lax.optimization_barrier(jnp.sum(jnp.where(entry_indices[None, :] == length - 1, gate_row, jnp.zeros_like(gate_row)), axis=1))
    current = last_gate + forget_log
    scores = jnp.einsum('hd,jhd->hj', query_h, key_h) * score_scale + (current[:, None] - gate_row)
    scores = jnp.where(entry_indices[None, :] < length, scores, -jnp.inf)
    own_score = lax.optimization_barrier(jnp.sum(query_h * key_new.astype(jnp.float32).reshape(heads, head_size), axis=1)) * score_scale
    row_peak = jnp.maximum(lax.optimization_barrier(jnp.max(scores, axis=1)), own_score)
    weights = jnp.exp(scores - row_peak[:, None])
    own_weight = jnp.exp(own_score - row_peak)
    denominator = lax.optimization_barrier(jnp.sum(weights, axis=1)) + own_weight
    weighted = jnp.einsum('hj,jhd->hd', bf16_round(weights), value_h)
    weighted = weighted + bf16_round(own_weight)[:, None] * value_new.astype(jnp.float32).reshape(heads, head_size)
    return (weighted / denominator[:, None]).astype(jnp.bfloat16).reshape(-1)

def reference(tokens, norm_attn, w_query, w_key, w_value, w_forget, forget_bias, w_output, key_cache, value_cache, gate_cache, lengths, norm_ffn, route_group, route_slot, route_weight, expert_gate, expert_up, expert_down, dense_gate, dense_up, dense_down, mix_vector):
    normed = rms_scale(tokens, norm_attn).astype(jnp.bfloat16)
    queries = jnp.dot(normed, w_query, preferred_element_type=jnp.float32).astype(jnp.bfloat16)
    key_new = jnp.dot(normed, w_key, preferred_element_type=jnp.float32).astype(jnp.bfloat16)
    value_new = jnp.dot(normed, w_value, preferred_element_type=jnp.float32).astype(jnp.bfloat16)
    forget_log = jax.nn.log_sigmoid(jnp.dot(normed, w_forget, preferred_element_type=jnp.float32) + forget_bias)
    attended = lax.map(attend_one, (queries, key_new, value_new, forget_log, key_cache, value_cache, gate_cache, lengths))
    head_block = HEADS * HEAD_DIM // N_TP
    head_parts = jnp.einsum('snr,nrd->snd', attended.astype(jnp.float32).reshape(STREAM_COUNT, N_TP, head_block), w_output.astype(jnp.float32).reshape(N_TP, head_block, D))
    attn_sum = lax.optimization_barrier(jnp.sum(bf16_round(head_parts), axis=1))
    residual = tokens.astype(jnp.float32) + attn_sum
    normed_ffn = rms_scale(residual, norm_ffn).astype(jnp.bfloat16)
    expert_ids = route_group[:, None] * EXPERTS_PER_GROUP + route_slot
    ff_block = EXPERT_FF // N_TP

    def expert_term(expert, running):
        coefficient = lax.optimization_barrier(jnp.sum(jnp.where(expert_ids == expert, route_weight, jnp.zeros_like(route_weight)), axis=1))
        gate_act = jnp.dot(normed_ffn, expert_gate[expert], preferred_element_type=jnp.float32)
        up_act = jnp.dot(normed_ffn, expert_up[expert], preferred_element_type=jnp.float32)
        hidden = (jax.nn.silu(gate_act) * up_act).astype(jnp.bfloat16)
        partial_value = jnp.einsum('snf,nfd->snd', hidden.astype(jnp.float32).reshape(STREAM_COUNT, N_TP, ff_block), expert_down[expert].astype(jnp.float32).reshape(N_TP, ff_block, D))
        result = bf16_round(lax.optimization_barrier(jnp.sum(bf16_round(partial_value), axis=1)))
        return running + coefficient[:, None] * result
    moe = lax.fori_loop(0, EXPERTS, expert_term, jnp.zeros((STREAM_COUNT, D), jnp.float32))
    feature_block = D // N_TP
    grouped = normed_ffn.astype(jnp.float32).reshape(STREAM_COUNT, N_TP, feature_block)
    gate_parts = jnp.einsum('snd,ndf->snf', grouped, dense_gate.astype(jnp.float32).reshape(N_TP, feature_block, DENSE_FF))
    up_parts = jnp.einsum('snd,ndf->snf', grouped, dense_up.astype(jnp.float32).reshape(N_TP, feature_block, DENSE_FF))
    gate_sum = lax.optimization_barrier(jnp.sum(bf16_round(gate_parts), axis=1))
    up_sum = lax.optimization_barrier(jnp.sum(bf16_round(up_parts), axis=1))
    dense_hidden = (jax.nn.silu(gate_sum) * up_sum).astype(jnp.bfloat16)
    dense_out = jnp.dot(dense_hidden, dense_down, preferred_element_type=jnp.float32)
    mix_gate = jax.nn.sigmoid(jnp.dot(normed_ffn.astype(jnp.float32), mix_vector, precision=lax.Precision.HIGHEST))
    return (residual + moe + mix_gate[:, None] * dense_out).astype(jnp.bfloat16)
```

```python
import functools

import jax
import jax.numpy as jnp
from jax import lax
from jax.experimental import pallas as pl
from jax.experimental.pallas import tpu as pltpu
from jax.sharding import Mesh
from jax.sharding import PartitionSpec as P

EXPERTS_PER_GROUP = 8
EP = ("ep_0", "ep_1")
EPS = 1e-06
F32 = jnp.float32
BF16 = jnp.bfloat16
NT = (((1,), (1,)), ((), ()))
VMEM = pl.BlockSpec(memory_space=pltpu.VMEM)
ANY = pl.BlockSpec(memory_space=pl.ANY)
MIB = 1 << 20


def rms_scale(rows, gain):
    rows = rows.astype(F32)
    return rows * lax.rsqrt(jnp.mean(rows * rows, axis=-1, keepdims=True) + EPS) * gain


def silu(v):
    return v * jax.nn.sigmoid(v)


def stacked(pair):
    return jnp.concatenate([pair[:, 0:1], pair[:, 1:2]], axis=0)


def attention_kernel(
    tokens_ref,
    gain_ref,
    forget_ref,
    bias_ref,
    gate_ref,
    length_ref,
    wq_hbm,
    wk_hbm,
    wv_hbm,
    wo_hbm,
    key_hbm,
    value_hbm,
    dg_hbm,
    du_hbm,
    dd_hbm,
    parts_ref,
    dense_ref,
    wqkv,
    wo,
    keys,
    values,
    dense,
    scores,
    weighted,
    w_sems,
    key_sems,
    value_sems,
):
    seqs, cache_len, width = keys.shape
    heads = 2
    half = width // heads
    rows = heads * seqs
    scale = half ** (-0.5)
    weight_copies = [
        pltpu.make_async_copy(src, wqkv.at[i], w_sems.at[i])
        for i, src in enumerate((wq_hbm, wk_hbm, wv_hbm))
    ]
    rows_in = dg_hbm.shape[0]
    hidden_in = dd_hbm.shape[0]
    late_copies = [
        pltpu.make_async_copy(wo_hbm, wo, w_sems.at[3]),
        pltpu.make_async_copy(dg_hbm, dense.at[pl.ds(0, rows_in)], w_sems.at[4]),
        pltpu.make_async_copy(du_hbm, dense.at[pl.ds(rows_in, rows_in)], w_sems.at[5]),
        pltpu.make_async_copy(
            dd_hbm.at[:, pl.ds(0, width)],
            dense.at[pl.ds(2 * rows_in, hidden_in)],
            w_sems.at[6],
        ),
        pltpu.make_async_copy(
            dd_hbm.at[:, pl.ds(width, width)],
            dense.at[pl.ds(2 * rows_in + hidden_in, hidden_in)],
            w_sems.at[7],
        ),
    ]
    key_copies = [
        pltpu.make_async_copy(key_hbm.at[s], keys.at[s], key_sems.at[s]) for s in range(seqs)
    ]
    value_copies = [
        pltpu.make_async_copy(value_hbm.at[s], values.at[s], value_sems.at[s]) for s in range(seqs)
    ]
    for copy in weight_copies + key_copies + late_copies + value_copies:
        copy.start()

    normed = rms_scale(tokens_ref[...], gain_ref[...]).astype(BF16)
    forget_logit = jnp.dot(normed, forget_ref[...], preferred_element_type=F32) + bias_ref[...]
    forget_log = stacked(jax.nn.log_sigmoid(forget_logit))
    qkv = []
    for i in range(3):
        weight_copies[i].wait()
        qkv.append(jnp.dot(normed, wqkv[i], preferred_element_type=F32).astype(BF16).astype(F32))
    query, key_new, value_new = qkv
    lane = lax.broadcasted_iota(jnp.int32, (1, width), 1)
    first_head = lane < half
    own = query * key_new
    own_score = scale * jnp.concatenate(
        [
            jnp.sum(jnp.where(first_head, own, 0.0), axis=1, keepdims=True),
            jnp.sum(jnp.where(first_head, 0.0, own), axis=1, keepdims=True),
        ],
        axis=0,
    )
    row8 = lax.broadcasted_iota(jnp.int32, (8, width), 0)
    lane8 = lax.broadcasted_iota(jnp.int32, (8, width), 1)
    head_mask = (row8 < heads) & ((lane8 < half) == (row8 == 0))
    for s in range(seqs):
        masked = jnp.where(head_mask, query[s : s + 1], 0.0).astype(BF16)
        key_copies[s].wait()
        result = lax.dot_general(masked, keys[s], NT, preferred_element_type=F32)
        scores[s : s + 1] = result[0:1]
        scores[seqs + s : seqs + s + 1] = result[1:2]
    gate = jnp.concatenate([gate_ref[:, 0, :], gate_ref[:, 1, :]], axis=0)
    length = jnp.concatenate([length_ref[...], length_ref[...]], axis=0)
    entry = lax.broadcasted_iota(jnp.int32, (rows, cache_len), 1)
    last_gate = jnp.sum(jnp.where(entry == length - 1, gate, 0.0), axis=1, keepdims=True)
    current = last_gate + forget_log
    score = scores[...] * scale + (current - gate)
    score = jnp.where(entry < length, score, -jnp.inf)
    peak = jnp.maximum(jnp.max(score, axis=1, keepdims=True), own_score)
    weights = jnp.exp(score - peak)
    own_weight = jnp.exp(own_score - peak)
    denominator = jnp.sum(weights, axis=1, keepdims=True) + own_weight
    scores[...] = weights
    for copy in late_copies:
        copy.wait()
    dense_block = dense[...]
    for i in range(dense_ref.shape[0]):
        dense_ref[i] = dense_block
    for s in range(seqs):
        pair = jnp.concatenate(
            [
                scores[s : s + 1],
                scores[seqs + s : seqs + s + 1],
                jnp.zeros((6, cache_len), F32),
            ],
            axis=0,
        ).astype(BF16)
        value_copies[s].wait()
        result = jnp.dot(pair, values[s], preferred_element_type=F32)
        weighted[s : s + 1] = jnp.where(first_head, result[0:1], result[1:2])
    own_weight = own_weight.astype(BF16).astype(F32)
    own_weight = jnp.where(first_head, own_weight[:seqs], own_weight[seqs:])
    denominator = jnp.where(first_head, denominator[:seqs], denominator[seqs:])
    attended = ((weighted[...] + own_weight * value_new) / denominator).astype(BF16)
    part = jnp.dot(attended, wo[...], preferred_element_type=F32).astype(BF16)
    for i in range(parts_ref.shape[0]):
        parts_ref[i] = part


def dispatch_kernel(
    parts_ref, tokens_ref, gain_ref, select_ref, mix_ref, out_ref, residual_ref, mix_gate_ref
):
    half = out_ref.shape[1]
    attn = parts_ref[0].astype(F32)
    for i in range(1, parts_ref.shape[0]):
        attn = attn + parts_ref[i].astype(F32)
    residual = tokens_ref[...].astype(F32) + attn
    residual_ref[...] = residual
    normed = rms_scale(residual, gain_ref[...]).astype(BF16)
    mix_gate_ref[...] = jax.nn.sigmoid(
        jnp.sum(normed.astype(F32) * mix_ref[...], axis=1, keepdims=True)
    )
    both = jnp.concatenate([normed[:, :half], normed[:, half:]], axis=0)
    out_ref[...] = jnp.dot(select_ref[...], both, preferred_element_type=F32).astype(BF16)


def expert_kernel(rows_ref, gate_ref, up_ref, down_ref, dense_ref, out_ref):
    rows, half = rows_ref.shape
    blocks, _, width = dense_ref.shape
    per_half = blocks // 2
    kb = half // per_half
    row = lax.broadcasted_iota(jnp.int32, (rows, 1), 0)
    second = lax.rem(row, 8) >= 4
    is_dense = lax.rem(row, 4) >= 2
    sums = [None, None]
    for t in range(blocks):
        h, b = divmod(t, per_half)
        part = jnp.dot(
            rows_ref[:, b * kb : (b + 1) * kb],
            jnp.concatenate(
                [
                    gate_ref[t * kb : (t + 1) * kb],
                    up_ref[t * kb : (t + 1) * kb],
                    dense_ref[t, 0:kb],
                    dense_ref[t, kb : 2 * kb],
                ],
                axis=1,
            ),
            preferred_element_type=F32,
        )
        sums[h] = part if sums[h] is None else sums[h] + part
    both = jnp.where(second, sums[1], sums[0])
    both = both.reshape(rows // 8, 8, 4 * width)
    both = (both + pltpu.roll(both, 4, 1)).reshape(rows, 4 * width)
    picked = silu(both[:, 0:width]) * both[:, width : 2 * width]
    dense = silu(both[:, 2 * width : 3 * width]) * both[:, 3 * width :]
    hidden = jnp.concatenate(
        [jnp.where(is_dense, 0.0, picked), jnp.where(is_dense, dense, 0.0)], axis=1
    ).astype(BF16)

    def block(t):
        dense_down = jnp.concatenate(
            [
                dense_ref[t, 2 * kb : 2 * kb + width],
                dense_ref[t, 2 * kb + width : 2 * kb + 2 * width],
            ],
            axis=1,
        )
        down = jnp.concatenate([down_ref[:, t * kb : (t + 1) * kb], dense_down], axis=0)
        return jnp.dot(hidden, down, preferred_element_type=F32)

    for b in range(per_half):
        out_ref[:, b * kb : (b + 1) * kb] = jnp.where(
            second, block(per_half + b), block(b)
        ).astype(BF16)


def combine_kernel(rows_ref, weight_ref, dense_mask_ref, mix_ref, out_ref):
    blocks, seqs, width = out_ref.shape
    mix = jnp.concatenate([mix_ref[...], mix_ref[...]], axis=0)
    weight = weight_ref[...] + dense_mask_ref[...] * mix
    high = weight.astype(BF16)
    low = (weight - high.astype(F32)).astype(BF16)
    rows = rows_ref[...]
    total = jnp.dot(high, rows, preferred_element_type=F32) + jnp.dot(
        low, rows, preferred_element_type=F32
    )
    per_half = blocks // 2
    for t in range(blocks):
        h, b = divmod(t, per_half)
        out_ref[t] = total[h * seqs : (h + 1) * seqs, b * width : (b + 1) * width].astype(BF16)


def limits(mib):
    return pltpu.CompilerParams(vmem_limit_bytes=mib * MIB)


def exchange(array, axis):
    return lax.all_to_all(array, axis, 0, 0, tiled=True)


def body(
    tokens,
    norm_attn,
    w_query,
    w_key,
    w_value,
    w_forget,
    forget_bias,
    w_output,
    key_cache,
    value_cache,
    gate_cache,
    lengths,
    norm_ffn,
    route_group,
    route_slot,
    route_weight,
    expert_gate,
    expert_up,
    expert_down,
    dense_gate,
    dense_up,
    dense_down,
    mix_vector,
):
    seqs, model_width = tokens.shape
    ep_count = lax.axis_size(EP)
    tp_count = lax.axis_size("tp")
    tp_position = lax.axis_index("tp")
    width_local = model_width // tp_count
    half = model_width // 2
    head_width = key_cache.shape[2]
    cache_len = key_cache.shape[1]
    dense_rows = 2 * dense_gate.shape[0] + 2 * dense_down.shape[0]

    parts, dense_out = pl.pallas_call(
        attention_kernel,
        name="attention",
        out_shape=(
            jax.ShapeDtypeStruct((tp_count, seqs, model_width), BF16),
            jax.ShapeDtypeStruct((tp_count, dense_rows, head_width), BF16),
        ),
        in_specs=[VMEM] * 6 + [ANY] * 9,
        out_specs=(VMEM, VMEM),
        scratch_shapes=[
            pltpu.VMEM((3, model_width, head_width), BF16),
            pltpu.VMEM((head_width, model_width), BF16),
            pltpu.VMEM((seqs, cache_len, head_width), BF16),
            pltpu.VMEM((seqs, cache_len, head_width), BF16),
            pltpu.VMEM((dense_rows, head_width), BF16),
            pltpu.VMEM((2 * seqs, cache_len), F32),
            pltpu.VMEM((seqs, head_width), F32),
            pltpu.SemaphoreType.DMA((8,)),
            pltpu.SemaphoreType.DMA((seqs,)),
            pltpu.SemaphoreType.DMA((seqs,)),
        ],
        compiler_params=limits(24),
        cost_estimate=pl.CostEstimate(flops=10**9, bytes_accessed=12 * MIB, transcendentals=40000),
    )(
        tokens,
        norm_attn.reshape(1, -1),
        w_forget,
        forget_bias.reshape(1, -1),
        gate_cache,
        lengths.reshape(-1, 1),
        w_query,
        w_key,
        w_value,
        w_output,
        key_cache,
        value_cache,
        dense_gate,
        dense_up,
        dense_down,
    )
    parts = exchange(parts, "tp")
    dense_weights = exchange(dense_out, "tp")

    picks = route_slot.shape[1]
    ids = (route_group[:, None] * EXPERTS_PER_GROUP + route_slot).reshape(-1)
    order = jnp.arange(seqs * picks, dtype=jnp.int32)
    earlier = jnp.sum(
        ((ids[:, None] == ids[None, :]) & (order[None, :] < order[:, None])).astype(jnp.int32),
        axis=1,
    )
    place = (ids * 8 + earlier).reshape(seqs, picks)
    row = jnp.arange(ep_count * 8, dtype=jnp.int32)
    row_half = (row // 4) % 2
    row_slot = row % 4
    row_place = (row // 8) * 8 + row_slot
    token = jnp.arange(2 * seqs, dtype=jnp.int32) % seqs
    token_half = jnp.arange(2 * seqs, dtype=jnp.int32) // seqs
    same_half = token_half[:, None] == row_half[None, :]
    hits = [
        same_half
        & (row_slot < 2)[None, :]
        & (jnp.tile(place[:, k], 2)[:, None] == row_place[None, :])
        for k in range(picks)
    ]
    dense_hit = (
        same_half
        & (row_slot >= 2)[None, :]
        & (token[:, None] == (tp_position * 2 + row_slot - 2)[None, :])
    )
    pick_weight = sum(
        jnp.where(hits[k], jnp.tile(route_weight[:, k], 2)[:, None], 0.0) for k in range(picks)
    )
    dense_mask = dense_hit.astype(F32)
    select = (functools.reduce(jnp.logical_or, hits) | dense_hit).astype(BF16).T

    outgoing, residual, mix_gate = pl.pallas_call(
        dispatch_kernel,
        name="dispatch",
        out_shape=(
            jax.ShapeDtypeStruct((ep_count * 8, half), BF16),
            jax.ShapeDtypeStruct((seqs, model_width), F32),
            jax.ShapeDtypeStruct((seqs, 1), F32),
        ),
        in_specs=[VMEM] * 5,
        out_specs=(VMEM, VMEM, VMEM),
        compiler_params=limits(8),
    )(parts, tokens, norm_ffn.reshape(1, -1), select, mix_vector.reshape(1, -1))
    arrived = exchange(outgoing.reshape(ep_count, 8, half), EP).reshape(ep_count * 8, half)
    results = pl.pallas_call(
        expert_kernel,
        name="experts",
        out_shape=jax.ShapeDtypeStruct((ep_count * 8, half), BF16),
        in_specs=[VMEM] * 5,
        out_specs=VMEM,
        compiler_params=limits(16),
    )(arrived, expert_gate[0], expert_up[0], expert_down[0], dense_weights)
    returned = exchange(results.reshape(ep_count, 8, half), EP).reshape(ep_count * 8, half)
    sums = pl.pallas_call(
        combine_kernel,
        name="combine",
        out_shape=jax.ShapeDtypeStruct((tp_count, seqs, width_local), BF16),
        in_specs=[VMEM] * 4,
        out_specs=VMEM,
        compiler_params=limits(8),
    )(returned, pick_weight, dense_mask, mix_gate)
    sums = exchange(sums, "tp")
    residual_mine = lax.dynamic_slice_in_dim(residual, tp_position * width_local, width_local, 1)
    return (residual_mine + jnp.sum(sums.astype(F32), axis=0)).astype(BF16)


def solution(mesh):
    split = Mesh(mesh.devices.reshape(8, 4, mesh.shape["tp"]), ("ep_0", "ep_1", "tp"))
    return jax.shard_map(
        body,
        mesh=split,
        in_specs=(
            P(EP, None),
            P(),
            P(None, "tp"),
            P(None, "tp"),
            P(None, "tp"),
            P(None, "tp"),
            P("tp"),
            P("tp", None),
            P(EP, None, "tp"),
            P(EP, None, "tp"),
            P(EP, "tp", None),
            P(EP),
            P(),
            P(EP),
            P(EP, None),
            P(EP, None),
            P(EP, None, "tp"),
            P(EP, None, "tp"),
            P(EP, "tp", None),
            P("tp", EP),
            P("tp", EP),
            P(EP, "tp"),
            P(),
        ),
        out_specs=P(EP, "tp"),
        check_vma=False,
    )
```

```python
import functools

import jax
import jax.numpy as jnp
from jax import lax
from jax.experimental import pallas as pl
from jax.experimental.pallas import tpu as pltpu
from jax.sharding import Mesh
from jax.sharding import PartitionSpec as P

EXPERTS_PER_GROUP = 8
EP = ("ep_0", "ep_1")
EPS = 1e-06
F32 = jnp.float32
BF16 = jnp.bfloat16
NT = (((1,), (1,)), ((), ()))
VMEM = pl.BlockSpec(memory_space=pltpu.VMEM)
SMEM = pl.BlockSpec(memory_space=pltpu.SMEM)
ANY = pl.BlockSpec(memory_space=pl.ANY)
MIB = 1 << 20


def rms_scale(rows, gain):
    rows = rows.astype(F32)
    return rows * lax.rsqrt(jnp.mean(rows * rows, axis=-1, keepdims=True) + EPS) * gain


def silu(v):
    return v * jax.nn.sigmoid(v)


def stacked(pair):
    return jnp.concatenate([pair[:, 0:1], pair[:, 1:2]], axis=0)


def attention_kernel(
    tokens_hbm,
    gain_hbm,
    forget_hbm,
    bias_hbm,
    gate_hbm,
    length_hbm,
    wq_hbm,
    wk_hbm,
    wv_hbm,
    wo_hbm,
    key_hbm,
    value_hbm,
    parts_ref,
    tokens_ref,
    gain_ref,
    forget_ref,
    bias_ref,
    gate_ref,
    length_ref,
    wqkv,
    wo,
    keys,
    values,
    scores,
    weighted,
    small_sems,
    w_sems,
    key_sems,
    value_sems,
):
    seqs, cache_len, width = keys.shape
    heads = 2
    half = width // heads
    rows = heads * seqs
    scale = half ** (-0.5)
    group = 4
    groups = seqs // group
    small = [
        pltpu.make_async_copy(src, dst, small_sems.at[i])
        for i, (src, dst) in enumerate(
            (
                (tokens_hbm, tokens_ref),
                (gain_hbm, gain_ref),
                (forget_hbm, forget_ref),
                (bias_hbm, bias_ref),
                (length_hbm, length_ref),
                (gate_hbm, gate_ref),
            )
        )
    ]
    weight_copies = [
        pltpu.make_async_copy(src, wqkv.at[i], w_sems.at[i])
        for i, src in enumerate((wq_hbm, wk_hbm, wv_hbm))
    ]
    output_copy = pltpu.make_async_copy(wo_hbm, wo, w_sems.at[3])
    part = lambda g: pl.ds(g * group, group)
    key_copies = [
        pltpu.make_async_copy(key_hbm.at[part(g)], keys.at[part(g)], key_sems.at[g])
        for g in range(groups)
    ]
    value_copies = [
        pltpu.make_async_copy(value_hbm.at[part(g)], values.at[part(g)], value_sems.at[g])
        for g in range(groups)
    ]
    for copy in small + weight_copies + key_copies + value_copies + [output_copy]:
        copy.start()
    for copy in small:
        copy.wait()
    normed = rms_scale(tokens_ref[...], gain_ref[...]).astype(BF16)
    forget_logit = (
        lax.dot_general(normed, forget_ref[...], NT, preferred_element_type=F32) + bias_ref[...]
    )
    forget_log = stacked(jax.nn.log_sigmoid(forget_logit))
    same = lax.broadcasted_iota(jnp.int32, (seqs, seqs), 0) == lax.broadcasted_iota(
        jnp.int32, (seqs, seqs), 1
    )
    length = jnp.sum(
        jnp.where(same, length_ref[...].astype(F32), 0.0), axis=1, keepdims=True
    ).astype(jnp.int32)
    length = jnp.concatenate([length, length], axis=0)
    gate = jnp.concatenate([gate_ref[:, 0, :], gate_ref[:, 1, :]], axis=0)
    entry = lax.broadcasted_iota(jnp.int32, (rows, cache_len), 1)
    last_gate = jnp.sum(jnp.where(entry == length - 1, gate, 0.0), axis=1, keepdims=True)
    current = last_gate + forget_log
    for copy in weight_copies:
        copy.wait()
    query, key_new, value_new = [
        jnp.dot(normed, wqkv[i], preferred_element_type=F32).astype(BF16).astype(F32)
        for i in range(3)
    ]
    lane = lax.broadcasted_iota(jnp.int32, (1, width), 1)
    first_head = lane < half
    own = query * key_new
    own_score = scale * jnp.concatenate(
        [
            jnp.sum(jnp.where(first_head, own, 0.0), axis=1, keepdims=True),
            jnp.sum(jnp.where(first_head, 0.0, own), axis=1, keepdims=True),
        ],
        axis=0,
    )
    row8 = lax.broadcasted_iota(jnp.int32, (8, width), 0)
    lane8 = lax.broadcasted_iota(jnp.int32, (8, width), 1)
    head_mask = (row8 < heads) & ((lane8 < half) == (row8 == 0))
    for g in range(groups):
        key_copies[g].wait()
        for s in range(g * group, (g + 1) * group):
            masked = jnp.where(head_mask, query[s : s + 1], 0.0).astype(BF16)
            result = lax.dot_general(masked, keys[s], NT, preferred_element_type=F32)
            scores[s : s + 1] = result[0:1]
            scores[seqs + s : seqs + s + 1] = result[1:2]
    score = scores[...] * scale + (current - gate)
    score = jnp.where(entry < length, score, -jnp.inf)
    peak = jnp.maximum(jnp.max(score, axis=1, keepdims=True), own_score)
    weights = jnp.exp(score - peak)
    own_weight = jnp.exp(own_score - peak)
    denominator = jnp.sum(weights, axis=1, keepdims=True) + own_weight
    scores[...] = weights
    for g in range(groups):
        value_copies[g].wait()
        for s in range(g * group, (g + 1) * group):
            pair = jnp.concatenate(
                [
                    scores[s : s + 1],
                    scores[seqs + s : seqs + s + 1],
                    jnp.zeros((6, cache_len), F32),
                ],
                axis=0,
            ).astype(BF16)
            result = jnp.dot(pair, values[s], preferred_element_type=F32)
            weighted[s : s + 1] = jnp.where(first_head, result[0:1], result[1:2])
    output_copy.wait()
    own_weight = own_weight.astype(BF16).astype(F32)
    own_weight = jnp.where(first_head, own_weight[:seqs], own_weight[seqs:])
    denominator = jnp.where(first_head, denominator[:seqs], denominator[seqs:])
    attended = ((weighted[...] + own_weight * value_new) / denominator).astype(BF16)
    head_part = jnp.dot(attended, wo[...], preferred_element_type=F32).astype(BF16)
    for i in range(parts_ref.shape[0]):
        parts_ref[i] = head_part


def dispatch_kernel(
    position_ref,
    parts_ref,
    tokens_ref,
    gain_ref,
    select_ref,
    mix_ref,
    pick_ref,
    dense_mask_ref,
    out_ref,
    residual_ref,
    high_ref,
    low_ref,
    scratch,
):
    half = out_ref.shape[1]
    width = residual_ref.shape[1]
    attn = parts_ref[0].astype(F32)
    for i in range(1, parts_ref.shape[0]):
        attn = attn + parts_ref[i].astype(F32)
    residual = tokens_ref[...].astype(F32) + attn
    scratch[...] = residual
    normed = rms_scale(residual, gain_ref[...]).astype(BF16)
    both = jnp.concatenate([normed[:, :half], normed[:, half:]], axis=0)
    out_ref[...] = jnp.dot(select_ref[...], both, preferred_element_type=F32).astype(BF16)
    mix = jax.nn.sigmoid(jnp.sum(normed.astype(F32) * mix_ref[...], axis=1, keepdims=True))
    weight = pick_ref[...] + dense_mask_ref[...] * jnp.concatenate([mix, mix], axis=0)
    high = weight.astype(BF16)
    high_ref[...] = high
    low_ref[...] = (weight - high.astype(F32)).astype(BF16)
    mine = pl.ds(pl.multiple_of(position_ref[0] * width, width), width)
    residual_ref[...] = scratch[:, mine]


def row_kinds(rows):
    row = lax.broadcasted_iota(jnp.int32, (rows, 1), 0)
    return lax.rem(row, 8) >= 4, lax.rem(row, 4) >= 2


def whole_rows(both):
    rows, width = both.shape
    both = both.reshape(rows // 8, 8, width)
    return (both + pltpu.roll(both, 4, 1)).reshape(rows, width)


def picked_kernel(rows_ref, gate_ref, up_ref, down_ref, out_ref):
    rows, half = rows_ref.shape
    width = gate_ref.shape[1]
    second, _ = row_kinds(rows)
    sums = []
    for h in range(2):
        weights = jnp.concatenate(
            [gate_ref[h * half : (h + 1) * half], up_ref[h * half : (h + 1) * half]], axis=1
        )
        sums.append(jnp.dot(rows_ref[...], weights, preferred_element_type=F32))
    both = whole_rows(jnp.where(second, sums[1], sums[0]))
    hidden = (silu(both[:, :width]) * both[:, width:]).astype(BF16)
    results = [
        jnp.dot(hidden, down_ref[:, h * half : (h + 1) * half], preferred_element_type=F32)
        for h in range(2)
    ]
    out_ref[...] = jnp.where(second, results[1], results[0]).astype(BF16)


def dense_kernel(position_ref, rows_ref, picked_ref, *refs):
    out_ref = refs[-1]
    dense_refs = refs[:-1]
    rows, half = rows_ref.shape
    blocks = len(dense_refs)
    width = dense_refs[0].shape[1]
    per_half = blocks // 2
    kb = half // per_half
    position = position_ref[0]
    second, is_dense = row_kinds(rows)
    places = []
    for k in range(blocks):
        t = lax.rem(position - k + blocks, blocks)
        b = lax.rem(t, per_half)
        places.append((pl.ds(pl.multiple_of(b * kb, kb), kb), second == (t >= per_half)))
    both = None
    for (inner, mine), dense_ref in zip(places, dense_refs):
        weights = jnp.concatenate([dense_ref[0:kb], dense_ref[kb : 2 * kb]], axis=1)
        part = jnp.dot(rows_ref[:, inner], weights, preferred_element_type=F32)
        part = jnp.where(mine, part, 0.0)
        both = part if both is None else both + part
    both = whole_rows(both)
    hidden = (silu(both[:, :width]) * both[:, width:]).astype(BF16)
    out_ref[...] = picked_ref[...]
    for (inner, mine), dense_ref in zip(places, dense_refs):
        down = jnp.concatenate(
            [
                dense_ref[2 * kb : 2 * kb + width],
                dense_ref[2 * kb + width : 2 * kb + 2 * width],
            ],
            axis=1,
        )
        result = jnp.dot(hidden, down, preferred_element_type=F32).astype(BF16)
        out_ref[:, inner] = jnp.where(mine & is_dense, result, out_ref[:, inner])


def combine_kernel(rows_ref, high_ref, low_ref, out_ref):
    blocks, seqs, width = out_ref.shape
    rows = rows_ref[...]
    total = jnp.dot(high_ref[...], rows, preferred_element_type=F32) + jnp.dot(
        low_ref[...], rows, preferred_element_type=F32
    )
    per_half = blocks // 2
    for t in range(blocks):
        h, b = divmod(t, per_half)
        out_ref[t] = total[h * seqs : (h + 1) * seqs, b * width : (b + 1) * width].astype(BF16)


def limits(mib):
    return pltpu.CompilerParams(vmem_limit_bytes=mib * MIB)


def exchange(array, axis):
    return lax.all_to_all(array, axis, 0, 0, tiled=True)


def body(
    tokens,
    norm_attn,
    w_query,
    w_key,
    w_value,
    w_forget,
    forget_bias,
    w_output,
    key_cache,
    value_cache,
    gate_cache,
    lengths,
    norm_ffn,
    route_group,
    route_slot,
    route_weight,
    expert_gate,
    expert_up,
    expert_down,
    dense_gate,
    dense_up,
    dense_down,
    mix_vector,
):
    seqs, model_width = tokens.shape
    ep_count = lax.axis_size(EP)
    tp_count = lax.axis_size("tp")
    tp_position = lax.axis_index("tp")
    width_local = model_width // tp_count
    half = model_width // 2
    head_width = key_cache.shape[2]
    cache_len = key_cache.shape[1]

    own_dense = jnp.concatenate(
        [dense_gate, dense_up, dense_down[:, :head_width], dense_down[:, head_width:]], axis=0
    )
    dense_weights = [own_dense]
    for k in range(1, tp_count):
        dense_weights.append(
            lax.ppermute(own_dense, "tp", [(i, (i + k) % tp_count) for i in range(tp_count)])
        )
    parts = pl.pallas_call(
        attention_kernel,
        name="attention",
        out_shape=jax.ShapeDtypeStruct((tp_count, seqs, model_width), BF16),
        in_specs=[ANY] * 12,
        out_specs=VMEM,
        scratch_shapes=[
            pltpu.VMEM((seqs, model_width), BF16),
            pltpu.VMEM((1, model_width), F32),
            pltpu.VMEM((2, model_width), BF16),
            pltpu.VMEM((1, 2), F32),
            pltpu.VMEM((seqs, 2, cache_len), F32),
            pltpu.VMEM((1, seqs), jnp.int32),
            pltpu.VMEM((3, model_width, head_width), BF16),
            pltpu.VMEM((head_width, model_width), BF16),
            pltpu.VMEM((seqs, cache_len, head_width), BF16),
            pltpu.VMEM((seqs, cache_len, head_width), BF16),
            pltpu.VMEM((2 * seqs, cache_len), F32),
            pltpu.VMEM((seqs, head_width), F32),
            pltpu.SemaphoreType.DMA((6,)),
            pltpu.SemaphoreType.DMA((4,)),
            pltpu.SemaphoreType.DMA((4,)),
            pltpu.SemaphoreType.DMA((4,)),
        ],
        compiler_params=limits(60),
        cost_estimate=pl.CostEstimate(flops=10**9, bytes_accessed=12 * MIB, transcendentals=40000),
    )(
        tokens,
        norm_attn.reshape(1, -1),
        w_forget.T,
        forget_bias.reshape(1, -1),
        gate_cache,
        lengths.reshape(1, -1),
        w_query,
        w_key,
        w_value,
        w_output,
        key_cache,
        value_cache,
    )
    parts = exchange(parts, "tp")

    picks = route_slot.shape[1]
    ids = (route_group[:, None] * EXPERTS_PER_GROUP + route_slot).reshape(-1)
    order = jnp.arange(seqs * picks, dtype=jnp.int32)
    earlier = jnp.sum(
        ((ids[:, None] == ids[None, :]) & (order[None, :] < order[:, None])).astype(jnp.int32),
        axis=1,
    )
    place = (ids * 8 + earlier).reshape(seqs, picks)
    row = jnp.arange(ep_count * 8, dtype=jnp.int32)
    row_half = (row // 4) % 2
    row_slot = row % 4
    row_place = (row // 8) * 8 + row_slot
    token = jnp.arange(2 * seqs, dtype=jnp.int32) % seqs
    token_half = jnp.arange(2 * seqs, dtype=jnp.int32) // seqs
    same_half = token_half[:, None] == row_half[None, :]
    hits = [
        same_half
        & (row_slot < 2)[None, :]
        & (jnp.tile(place[:, k], 2)[:, None] == row_place[None, :])
        for k in range(picks)
    ]
    dense_hit = (
        same_half
        & (row_slot >= 2)[None, :]
        & (token[:, None] == (tp_position * 2 + row_slot - 2)[None, :])
    )
    pick_weight = sum(
        jnp.where(hits[k], jnp.tile(route_weight[:, k], 2)[:, None], 0.0) for k in range(picks)
    )
    dense_mask = dense_hit.astype(F32)
    select = (functools.reduce(jnp.logical_or, hits) | dense_hit).astype(BF16).T

    position = tp_position.reshape(1)
    dispatch = pl.pallas_call(
        dispatch_kernel,
        name="dispatch",
        out_shape=(
            jax.ShapeDtypeStruct((ep_count * 8, half), BF16),
            jax.ShapeDtypeStruct((seqs, width_local), F32),
            jax.ShapeDtypeStruct((2 * seqs, ep_count * 8), BF16),
            jax.ShapeDtypeStruct((2 * seqs, ep_count * 8), BF16),
        ),
        in_specs=[SMEM] + [VMEM] * 7,
        out_specs=(VMEM, VMEM, VMEM, VMEM),
        scratch_shapes=[pltpu.VMEM((seqs, model_width), F32)],
        compiler_params=limits(8),
    )
    outgoing, residual, high, low = dispatch(
        position,
        parts,
        tokens,
        norm_ffn.reshape(1, -1),
        select,
        mix_vector.reshape(1, -1),
        pick_weight,
        dense_mask,
    )
    arrived = exchange(outgoing.reshape(ep_count, 8, half), EP).reshape(ep_count * 8, half)
    results = pl.pallas_call(
        picked_kernel,
        name="picked",
        out_shape=jax.ShapeDtypeStruct((ep_count * 8, half), BF16),
        in_specs=[VMEM] * 4,
        out_specs=VMEM,
        compiler_params=limits(8),
    )(arrived, expert_gate[0], expert_up[0], expert_down[0])
    results = pl.pallas_call(
        dense_kernel,
        name="dense",
        out_shape=jax.ShapeDtypeStruct((ep_count * 8, half), BF16),
        in_specs=[SMEM] + [VMEM] * (2 + tp_count),
        out_specs=VMEM,
        compiler_params=limits(8),
    )(position, arrived, results, *dense_weights)
    returned = exchange(results.reshape(ep_count, 8, half), EP).reshape(ep_count * 8, half)
    sums = pl.pallas_call(
        combine_kernel,
        name="combine",
        out_shape=jax.ShapeDtypeStruct((tp_count, seqs, width_local), BF16),
        in_specs=[VMEM] * 3,
        out_specs=VMEM,
        compiler_params=limits(8),
    )(returned, high, low)
    sums = exchange(sums, "tp")
    return (residual + jnp.sum(sums.astype(F32), axis=0)).astype(BF16)


def solution(mesh):
    split = Mesh(mesh.devices.reshape(8, 4, mesh.shape["tp"]), ("ep_0", "ep_1", "tp"))
    return jax.shard_map(
        body,
        mesh=split,
        in_specs=(
            P(EP, None),
            P(),
            P(None, "tp"),
            P(None, "tp"),
            P(None, "tp"),
            P(None, "tp"),
            P("tp"),
            P("tp", None),
            P(EP, None, "tp"),
            P(EP, None, "tp"),
            P(EP, "tp", None),
            P(EP),
            P(),
            P(EP),
            P(EP, None),
            P(EP, None),
            P(EP, None, "tp"),
            P(EP, None, "tp"),
            P(EP, "tp", None),
            P("tp", EP),
            P("tp", EP),
            P(EP, "tp"),
            P(),
        ),
        out_specs=P(EP, "tp"),
        check_vma=False,
    )
```

```python
import jax
import jax.numpy as jnp
from jax import lax
from jax.experimental import pallas as pl
from jax.experimental.pallas import tpu as pltpu
from jax.sharding import Mesh
from jax.sharding import PartitionSpec as P

EXPERTS_PER_GROUP = 8
EXPERTS = 32
EP = ("ep_0", "ep_1")
EPS = 1e-06
F32 = jnp.float32
BF16 = jnp.bfloat16
NT = (((1,), (1,)), ((), ()))
VMEM = pl.BlockSpec(memory_space=pltpu.VMEM)
SMEM = pl.BlockSpec(memory_space=pltpu.SMEM)
ANY = pl.BlockSpec(memory_space=pl.ANY)
MIB = 1 << 20


def rms_scale(rows, gain):
    rows = rows.astype(F32)
    return rows * lax.rsqrt(jnp.mean(rows * rows, axis=-1, keepdims=True) + EPS) * gain


def silu(v):
    return v * jax.nn.sigmoid(v)


def stacked(pair):
    return jnp.concatenate([pair[:, 0:1], pair[:, 1:2]], axis=0)


def attention_kernel(
    tokens_hbm,
    gain_hbm,
    forget_hbm,
    bias_hbm,
    gate_hbm,
    length_hbm,
    group_hbm,
    slot_hbm,
    route_weight_hbm,
    wq_hbm,
    wk_hbm,
    wv_hbm,
    wo_hbm,
    key_hbm,
    value_hbm,
    parts_ref,
    table_ref,
    tokens_ref,
    gain_ref,
    forget_ref,
    bias_ref,
    gate_ref,
    length_ref,
    group_ref,
    slot_ref,
    route_weight_ref,
    wqkv,
    wo,
    keys,
    values,
    scores,
    weighted,
    small_sems,
    w_sems,
    key_sems,
    value_sems,
):
    seqs, cache_len, width = keys.shape
    heads = 2
    half = width // heads
    rows = heads * seqs
    scale = half ** (-0.5)
    key_group, value_group = 16, 16
    small = [
        pltpu.make_async_copy(src, dst, small_sems.at[i])
        for i, (src, dst) in enumerate(
            (
                (tokens_hbm, tokens_ref),
                (gain_hbm, gain_ref),
                (forget_hbm, forget_ref),
                (bias_hbm, bias_ref),
                (length_hbm, length_ref),
                (gate_hbm, gate_ref),
                (group_hbm, group_ref),
                (slot_hbm, slot_ref),
                (route_weight_hbm, route_weight_ref),
            )
        )
    ]
    weight_copies = [
        pltpu.make_async_copy(src, wqkv.at[i], w_sems.at[i])
        for i, src in enumerate((wq_hbm, wk_hbm, wv_hbm))
    ]
    output_copy = pltpu.make_async_copy(wo_hbm, wo, w_sems.at[3])
    part = lambda g, n: pl.ds(g * n, n)
    key_copies = [
        pltpu.make_async_copy(key_hbm.at[part(g, key_group)], keys.at[part(g, key_group)], key_sems.at[g])
        for g in range(seqs // key_group)
    ]
    value_copies = [
        pltpu.make_async_copy(value_hbm.at[part(g, value_group)], values.at[part(g, value_group)], value_sems.at[g])
        for g in range(seqs // value_group)
    ]
    for copy in small + weight_copies + key_copies + value_copies + [output_copy]:
        copy.start()
    for copy in small:
        copy.wait()
    normed = rms_scale(tokens_ref[...], gain_ref[...]).astype(BF16)
    forget_logit = (
        lax.dot_general(normed, forget_ref[...], NT, preferred_element_type=F32) + bias_ref[...]
    )
    forget_log = stacked(jax.nn.log_sigmoid(forget_logit))
    length = column_of(length_ref[...]).astype(jnp.int32)
    length = jnp.concatenate([length, length], axis=0)
    gate = jnp.concatenate([gate_ref[:, 0, :], gate_ref[:, 1, :]], axis=0)
    entry = lax.broadcasted_iota(jnp.int32, (rows, cache_len), 1)
    last_gate = jnp.sum(jnp.where(entry == length - 1, gate, 0.0), axis=1, keepdims=True)
    current = last_gate + forget_log
    for copy in weight_copies:
        copy.wait()
    query, key_new, value_new = [
        jnp.dot(normed, wqkv[i], preferred_element_type=F32).astype(BF16).astype(F32)
        for i in range(3)
    ]
    lane = lax.broadcasted_iota(jnp.int32, (1, width), 1)
    first_head = lane < half
    own = query * key_new
    own_score = scale * jnp.concatenate(
        [
            jnp.sum(jnp.where(first_head, own, 0.0), axis=1, keepdims=True),
            jnp.sum(jnp.where(first_head, 0.0, own), axis=1, keepdims=True),
        ],
        axis=0,
    )
    row8 = lax.broadcasted_iota(jnp.int32, (8, width), 0)
    lane8 = lax.broadcasted_iota(jnp.int32, (8, width), 1)
    masks = [
        (row8 // heads == i) & ((lane8 < half) == (lax.rem(row8, heads) == 0)) for i in range(2)
    ]
    place_columns = routing_places(group_ref[...] * EXPERTS_PER_GROUP + slot_ref[...])
    combine_table(place_columns, route_weight_ref[...], table_ref)
    tail = jnp.zeros((seqs, width), F32)
    for k, place in enumerate(place_columns):
        tail = tail + jnp.where(lane == k, place.astype(F32), 0.0)
    tail = tail.astype(BF16)
    for g in range(seqs // key_group):
        key_copies[g].wait()
        for s in range(g * key_group, (g + 1) * key_group, 2):
            masked = jnp.concatenate(
                [jnp.where(masks[i], query[s + i : s + i + 1], 0.0) for i in range(2)], axis=1
            ).astype(BF16)
            pair = jnp.concatenate([keys[s], keys[s + 1]], axis=1)
            result = lax.dot_general(masked, pair, NT, preferred_element_type=F32)
            for i in range(2):
                for h in range(heads):
                    scores[h * seqs + s + i : h * seqs + s + i + 1] = result[
                        heads * i + h : heads * i + h + 1
                    ]
    score = scores[...] * scale + (current - gate)
    score = jnp.where(entry < length, score, -jnp.inf)
    peak = jnp.maximum(jnp.max(score, axis=1, keepdims=True), own_score)
    weights = jnp.exp(score - peak)
    own_weight = jnp.exp(own_score - peak)
    denominator = jnp.sum(weights, axis=1, keepdims=True) + own_weight
    scores[...] = weights
    for g in range(seqs // value_group):
        value_copies[g].wait()
        for s in range(g * value_group, (g + 1) * value_group, 2):
            four = jnp.concatenate(
                [
                    scores[h * seqs + s + i : h * seqs + s + i + 1]
                    for i in range(2)
                    for h in range(heads)
                ]
                + [jnp.zeros((4, cache_len), F32)],
                axis=0,
            ).astype(BF16)
            pair = jnp.concatenate([values[s], values[s + 1]], axis=1)
            result = jnp.dot(four, pair, preferred_element_type=F32)
            for i in range(2):
                mine = result[heads * i : heads * i + heads, i * width : (i + 1) * width]
                weighted[s + i : s + i + 1] = jnp.where(first_head, mine[0:1], mine[1:2])
    output_copy.wait()
    own_weight = own_weight.astype(BF16).astype(F32)
    own_weight = jnp.where(first_head, own_weight[:seqs], own_weight[seqs:])
    denominator = jnp.where(first_head, denominator[:seqs], denominator[seqs:])
    attended = ((weighted[...] + own_weight * value_new) / denominator).astype(BF16)
    head_part = jnp.dot(attended, wo[...], preferred_element_type=F32).astype(BF16)
    model_width = head_part.shape[1]
    for i in range(parts_ref.shape[0]):
        parts_ref[i, :, 0:model_width] = head_part
        parts_ref[i, :, model_width:] = tail


def column_of(row):
    n = row.shape[1]
    same = lax.broadcasted_iota(jnp.int32, (n, n), 0) == lax.broadcasted_iota(
        jnp.int32, (n, n), 1
    )
    return jnp.sum(jnp.where(same, row.astype(F32), 0.0), axis=1, keepdims=True)


def routing_places(ids):
    picks, seqs = ids.shape
    columns = [column_of(ids[k : k + 1]) for k in range(picks)]
    down = lax.broadcasted_iota(jnp.int32, (seqs, seqs), 0)
    across = lax.broadcasted_iota(jnp.int32, (seqs, seqs), 1)
    rows = [ids[k : k + 1].astype(F32) for k in range(picks)]
    places = []
    for column in columns:
        before = jnp.zeros((seqs, 1), F32)
        for row in rows:
            hit = (column == row) & (across < down)
            before = before + jnp.sum(jnp.where(hit, 1.0, 0.0), axis=1, keepdims=True)
        places.append((column * 8 + before).astype(jnp.int32))
    return places


def select_table(place_rows, position, rows):
    seqs = place_rows[0].shape[1]
    row = lax.broadcasted_iota(jnp.int32, (rows, 2 * seqs), 0)
    column = lax.broadcasted_iota(jnp.int32, (rows, 2 * seqs), 1)
    slot = row & 3
    row_place = (row & ~7) + slot
    token = column & (seqs - 1)
    hit = (slot >= 2) & (token == position * 2 + slot - 2)
    for place in place_rows:
        places = jnp.concatenate([place, place], axis=1)
        hit = hit | ((slot < 2) & (places == row_place))
    same_half = ((row >> 2) & 1) == (column >= seqs).astype(jnp.int32)
    return jnp.where(hit & same_half, 1.0, 0.0).astype(BF16)


def combine_table(place_columns, weight_rows, table_ref):
    seqs = place_columns[0].shape[0]
    wide = table_ref.shape[1]
    row = lax.broadcasted_iota(jnp.int32, (2 * seqs, wide), 0)
    column = lax.broadcasted_iota(jnp.int32, (2 * seqs, wide), 1)
    slot = column & 3
    source = (column >> 3) & 7
    expert_place = ((column >> 6) << 3) + slot
    same_half = ((column >> 2) & 1) == (row >= seqs).astype(jnp.int32)
    weight = jnp.zeros((2 * seqs, wide), F32)
    for k, place in enumerate(place_columns):
        places = jnp.concatenate([place, place], axis=0)
        value = column_of(weight_rows[k : k + 1])
        value = jnp.concatenate([value, value], axis=0)
        weight = weight + jnp.where(
            same_half & (slot < 2) & (places == expert_place), value, 0.0
        )
    high = weight.astype(BF16)
    table_ref[0 : 2 * seqs] = high
    table_ref[2 * seqs : 4 * seqs] = (weight - high.astype(F32)).astype(BF16)
    dense = same_half & (slot >= 2) & ((row & (seqs - 1)) == source * 2 + slot - 2)
    table_ref[4 * seqs : 6 * seqs] = jnp.where(dense, 1.0, 0.0).astype(BF16)


def dispatch_kernel(
    position_ref,
    parts_ref,
    tokens_ref,
    gain_ref,
    mix_ref,
    out_ref,
    residual_ref,
    mix_gate_ref,
    scratch,
):
    half = out_ref.shape[1]
    width = residual_ref.shape[1]
    model_width = tokens_ref.shape[1]
    seqs = tokens_ref.shape[0]
    columns = parts_ref[0, :, model_width:].astype(F32)
    same = lax.broadcasted_iota(jnp.int32, (seqs, seqs), 0) == lax.broadcasted_iota(
        jnp.int32, (seqs, seqs), 1
    )
    place_rows = [
        jnp.sum(jnp.where(same, columns[:, k : k + 1], 0.0), axis=0, keepdims=True).astype(
            jnp.int32
        )
        for k in range(2)
    ]
    select = select_table(place_rows, position_ref[0], out_ref.shape[0])
    attn = parts_ref[0, :, 0:model_width].astype(F32)
    for i in range(1, parts_ref.shape[0]):
        attn = attn + parts_ref[i, :, 0:model_width].astype(F32)
    residual = tokens_ref[...].astype(F32) + attn
    scratch[...] = residual
    normed = rms_scale(residual, gain_ref[...]).astype(BF16)
    both = jnp.concatenate([normed[:, :half], normed[:, half:]], axis=0)
    mix_gate_ref[...] = jax.nn.sigmoid(
        jnp.sum(normed.astype(F32) * mix_ref[...], axis=1, keepdims=True)
    )
    mine = pl.ds(pl.multiple_of(position_ref[0] * width, width), width)
    residual_ref[...] = scratch[:, mine]
    out_ref[...] = jnp.dot(select, both, preferred_element_type=F32).astype(BF16)


def row_kinds(rows):
    row = lax.broadcasted_iota(jnp.int32, (rows, 1), 0)
    return lax.rem(row, 8) >= 4, lax.rem(row, 4) >= 2


def whole_rows(both):
    rows, width = both.shape
    both = both.reshape(rows // 8, 8, width)
    return (both + pltpu.roll(both, 4, 1)).reshape(rows, width)


def picked_kernel(rows_ref, gate_ref, up_ref, hidden_ref):
    rows, half = rows_ref.shape
    width = gate_ref.shape[1]
    second, is_dense = row_kinds(rows)
    sums = []
    for h in range(2):
        weights = jnp.concatenate(
            [gate_ref[h * half : (h + 1) * half], up_ref[h * half : (h + 1) * half]], axis=1
        )
        sums.append(jnp.dot(rows_ref[...], weights, preferred_element_type=F32))
    both = whole_rows(jnp.where(second, sums[1], sums[0]))
    hidden = silu(both[:, :width]) * both[:, width:]
    hidden_ref[...] = jnp.where(is_dense, 0.0, hidden).astype(BF16)


LATE = (1, 2, 3, 4)


def dense_kernel(position_ref, rows_ref, picked_ref, down_ref, *refs):
    out_ref, late, sems = refs[-3:]
    operands = refs[:-3]
    blocks = len(operands)
    copies = [
        pltpu.make_async_copy(operands[k], late.at[i], sems.at[i]) for i, k in enumerate(LATE)
    ]
    for copy in copies:
        copy.start()
    pieces = {k: operands[k] for k in range(blocks) if k not in LATE}
    pieces.update({k: late.at[i] for i, k in enumerate(LATE)})
    rows, half = rows_ref.shape
    width = late.shape[2]
    per_half = blocks // 2
    kb = half // per_half
    position = position_ref[0]
    second, is_dense = row_kinds(rows)
    both = None
    for k, piece in pieces.items():
        if k == LATE[0]:
            for copy in copies:
                copy.wait()
        t = lax.rem(position - k + blocks, blocks)
        inner = pl.ds(pl.multiple_of(lax.rem(t, per_half) * kb, kb), kb)
        weights = jnp.concatenate([piece[0:kb], piece[kb : 2 * kb]], axis=1)
        part = jnp.dot(rows_ref[:, inner], weights, preferred_element_type=F32)
        part = jnp.where(second == (t >= per_half), part, 0.0)
        both = part if both is None else both + part
    both = whole_rows(both)
    hidden = silu(both[:, :width]) * both[:, width:]
    hidden = jnp.concatenate(
        [picked_ref[...], jnp.where(is_dense, hidden, 0.0).astype(BF16)], axis=1
    )
    for k, piece in pieces.items():
        t = lax.rem(position - k + blocks, blocks)
        dense_down = jnp.concatenate(
            [piece[2 * kb : 2 * kb + width], piece[2 * kb + width : 2 * kb + 2 * width]], axis=1
        )
        whole = pl.ds(pl.multiple_of(t * kb, kb), kb)
        down = jnp.concatenate([down_ref[:, whole], dense_down], axis=0)
        result = jnp.dot(hidden, down, preferred_element_type=F32)
        result = jnp.where(second, result[:, width:], result[:, :width]).astype(BF16)
        out_ref[:, t] = result.reshape(rows // 8, 8, width)


def combine_kernel(rows_ref, table_ref, mix_ref, residual_ref, out_ref):
    seqs = mix_ref.shape[0]
    width = rows_ref.shape[1]
    sums = jnp.dot(table_ref[...], rows_ref[...], preferred_element_type=F32)
    mix = mix_ref[...]
    for p in range(2):
        picked = sums[p * seqs : (p + 1) * seqs] + sums[(2 + p) * seqs : (3 + p) * seqs]
        dense = sums[(4 + p) * seqs : (5 + p) * seqs]
        columns = slice(p * width, (p + 1) * width)
        out_ref[:, columns] = (residual_ref[:, columns] + picked + mix * dense).astype(BF16)


def limits(mib):
    return pltpu.CompilerParams(vmem_limit_bytes=mib * MIB)


def exchange(array, axis):
    return lax.all_to_all(array, axis, 0, 0, tiled=True)


def attention_call(*operands):
    tokens, key_cache = operands[0], operands[13]
    seqs, model_width = tokens.shape
    _, cache_len, head_width = key_cache.shape
    tp_count = 8
    return pl.pallas_call(
        attention_kernel,
        name="attention",
        out_shape=(
            jax.ShapeDtypeStruct((tp_count, seqs, model_width + head_width), BF16),
            jax.ShapeDtypeStruct((6 * seqs, EXPERTS * 8 * tp_count), BF16),
        ),
        in_specs=[ANY] * 15,
        out_specs=(VMEM, VMEM),
        scratch_shapes=[
            pltpu.VMEM((seqs, model_width), BF16),
            pltpu.VMEM((1, model_width), F32),
            pltpu.VMEM((2, model_width), BF16),
            pltpu.VMEM((1, 2), F32),
            pltpu.VMEM((seqs, 2, cache_len), F32),
            pltpu.VMEM((1, seqs), jnp.int32),
            pltpu.VMEM((1, seqs), jnp.int32),
            pltpu.VMEM((2, seqs), jnp.int32),
            pltpu.VMEM((2, seqs), F32),
            pltpu.VMEM((3, model_width, head_width), BF16),
            pltpu.VMEM((head_width, model_width), BF16),
            pltpu.VMEM((seqs, cache_len, head_width), BF16),
            pltpu.VMEM((seqs, cache_len, head_width), BF16),
            pltpu.VMEM((2 * seqs, cache_len), F32),
            pltpu.VMEM((seqs, head_width), F32),
            pltpu.SemaphoreType.DMA((9,)),
            pltpu.SemaphoreType.DMA((4,)),
            pltpu.SemaphoreType.DMA((16,)),
            pltpu.SemaphoreType.DMA((16,)),
        ],
        compiler_params=limits(60),
        cost_estimate=pl.CostEstimate(flops=10**9, bytes_accessed=12 * MIB, transcendentals=40000),
    )(*operands)


def body(
    tokens,
    norm_attn,
    w_query,
    w_key,
    w_value,
    w_forget,
    forget_bias,
    w_output,
    key_cache,
    value_cache,
    gate_cache,
    lengths,
    norm_ffn,
    route_group,
    route_slot,
    route_weight,
    expert_gate,
    expert_up,
    expert_down,
    dense_gate,
    dense_up,
    dense_down,
    mix_vector,
):
    seqs, model_width = tokens.shape
    ep_count = lax.axis_size(EP)
    tp_count = lax.axis_size("tp")
    tp_position = lax.axis_index("tp")
    width_local = model_width // tp_count
    half = model_width // 2
    head_width = key_cache.shape[2]

    own_dense = jnp.concatenate(
        [dense_gate, dense_up, dense_down[:, :head_width], dense_down[:, head_width:]], axis=0
    )
    dense_weights = [own_dense]
    for k in range(1, tp_count):
        dense_weights.append(
            lax.ppermute(own_dense, "tp", [(i, (i + k) % tp_count) for i in range(tp_count)])
        )
    parts, table = attention_call(
        tokens,
        norm_attn.reshape(1, -1),
        w_forget.T,
        forget_bias.reshape(1, -1),
        gate_cache,
        lengths.reshape(1, -1),
        route_group.reshape(1, -1),
        route_slot.T,
        route_weight.T,
        w_query,
        w_key,
        w_value,
        w_output,
        key_cache,
        value_cache,
    )
    parts = exchange(parts, "tp")

    position = tp_position.reshape(1)
    row_count = ep_count * 8
    wide = row_count * tp_count
    dispatch = pl.pallas_call(
        dispatch_kernel,
        name="dispatch",
        out_shape=(
            jax.ShapeDtypeStruct((row_count, half), BF16),
            jax.ShapeDtypeStruct((seqs, width_local), F32),
            jax.ShapeDtypeStruct((seqs, 1), F32),
        ),
        in_specs=[SMEM] + [VMEM] * 4,
        out_specs=(VMEM, VMEM, VMEM),
        scratch_shapes=[pltpu.VMEM((seqs, model_width), F32)],
        compiler_params=limits(8),
    )
    outgoing, residual, mix_gate = dispatch(
        position,
        parts,
        tokens,
        norm_ffn.reshape(1, -1),
        mix_vector.reshape(1, -1),
    )
    arrived = exchange(outgoing.reshape(ep_count, 8, half), EP).reshape(row_count, half)
    hidden = pl.pallas_call(
        picked_kernel,
        name="picked",
        out_shape=jax.ShapeDtypeStruct((row_count, head_width), BF16),
        in_specs=[VMEM] * 3,
        out_specs=VMEM,
        compiler_params=limits(8),
    )(arrived, expert_gate[0], expert_up[0])
    results = pl.pallas_call(
        dense_kernel,
        name="dense",
        out_shape=jax.ShapeDtypeStruct((ep_count, tp_count, 8, width_local // 2), BF16),
        in_specs=[SMEM] + [VMEM] * 3 + [ANY if k in LATE else VMEM for k in range(tp_count)],
        out_specs=VMEM,
        scratch_shapes=[
            pltpu.VMEM((len(LATE), *own_dense.shape), BF16),
            pltpu.SemaphoreType.DMA((len(LATE),)),
        ],
        compiler_params=limits(8),
    )(position, arrived, hidden, expert_down[0], *dense_weights)
    returned = exchange(
        results.reshape(ep_count * tp_count, 8, width_local // 2), (*EP, "tp")
    ).reshape(wide, width_local // 2)
    return pl.pallas_call(
        combine_kernel,
        name="combine",
        out_shape=jax.ShapeDtypeStruct((seqs, width_local), BF16),
        in_specs=[VMEM] * 4,
        out_specs=VMEM,
        compiler_params=limits(8),
    )(returned, table, mix_gate, residual)


def solution(mesh):
    split = Mesh(mesh.devices.reshape(8, 4, mesh.shape["tp"]), ("ep_0", "ep_1", "tp"))
    return jax.shard_map(
        body,
        mesh=split,
        in_specs=(
            P(EP, None),
            P(),
            P(None, "tp"),
            P(None, "tp"),
            P(None, "tp"),
            P(None, "tp"),
            P("tp"),
            P("tp", None),
            P(EP, None, "tp"),
            P(EP, None, "tp"),
            P(EP, "tp", None),
            P(EP),
            P(),
            P(EP),
            P(EP, None),
            P(EP, None),
            P(EP, None, "tp"),
            P(EP, None, "tp"),
            P(EP, "tp", None),
            P("tp", EP),
            P("tp", EP),
            P(EP, "tp"),
            P(),
        ),
        out_specs=P(EP, "tp"),
        check_vma=False,
    )
```

```python
import jax
import jax.numpy as jnp
from jax import lax
from jax.experimental import pallas as pl
from jax.experimental.pallas import tpu as pltpu
from jax.sharding import Mesh
from jax.sharding import PartitionSpec as P

EXPERTS_PER_GROUP = 8
EXPERTS = 32
EP = ("ep_0", "ep_1")
TP = ("y", "core")
EPS = 1e-06
F32 = jnp.float32
BF16 = jnp.bfloat16
NT = (((1,), (1,)), ((), ()))
VMEM = pl.BlockSpec(memory_space=pltpu.VMEM)
SMEM = pl.BlockSpec(memory_space=pltpu.SMEM)
ANY = pl.BlockSpec(memory_space=pl.ANY)
MIB = 1 << 20


def rms_scale(rows, gain):
    rows = rows.astype(F32)
    return rows * lax.rsqrt(jnp.mean(rows * rows, axis=-1, keepdims=True) + EPS) * gain


def silu(v):
    return v * jax.nn.sigmoid(v)


def stacked(pair):
    return jnp.concatenate([pair[:, 0:1], pair[:, 1:2]], axis=0)


def attention_kernel(
    tokens_hbm,
    gain_hbm,
    forget_hbm,
    bias_hbm,
    gate_hbm,
    length_hbm,
    group_hbm,
    slot_hbm,
    route_weight_hbm,
    wq_hbm,
    wk_hbm,
    wv_hbm,
    wo_hbm,
    key_hbm,
    value_hbm,
    parts_ref,
    table_hbm,
    tokens_ref,
    gain_ref,
    forget_ref,
    bias_ref,
    gate_ref,
    length_ref,
    group_ref,
    slot_ref,
    route_weight_ref,
    table_ref,
    wqkv,
    wo,
    keys,
    values,
    scores,
    weighted,
    small_sems,
    w_sems,
    key_sems,
    value_sems,
):
    seqs, cache_len, width = keys.shape
    heads = 2
    half = width // heads
    rows = heads * seqs
    scale = half ** (-0.5)
    key_group, value_group = 16, 16
    small = [
        pltpu.make_async_copy(src, dst, small_sems.at[i])
        for i, (src, dst) in enumerate(
            (
                (tokens_hbm, tokens_ref),
                (gain_hbm, gain_ref),
                (forget_hbm, forget_ref),
                (bias_hbm, bias_ref),
                (length_hbm, length_ref),
                (gate_hbm, gate_ref),
                (group_hbm, group_ref),
                (slot_hbm, slot_ref),
                (route_weight_hbm, route_weight_ref),
            )
        )
    ]
    weight_copies = [
        pltpu.make_async_copy(src, wqkv.at[i], w_sems.at[i])
        for i, src in enumerate((wq_hbm, wk_hbm, wv_hbm))
    ]
    output_copy = pltpu.make_async_copy(wo_hbm, wo, w_sems.at[3])
    part = lambda g, n: pl.ds(g * n, n)
    key_copies = [
        pltpu.make_async_copy(key_hbm.at[part(g, key_group)], keys.at[part(g, key_group)], key_sems.at[g])
        for g in range(seqs // key_group)
    ]
    value_copies = [
        pltpu.make_async_copy(value_hbm.at[part(g, value_group)], values.at[part(g, value_group)], value_sems.at[g])
        for g in range(seqs // value_group)
    ]
    for copy in small + weight_copies + key_copies + value_copies + [output_copy]:
        copy.start()
    for copy in small:
        copy.wait()
    normed = rms_scale(tokens_ref[...], gain_ref[...]).astype(BF16)
    forget_logit = (
        lax.dot_general(normed, forget_ref[...], NT, preferred_element_type=F32) + bias_ref[...]
    )
    forget_log = stacked(jax.nn.log_sigmoid(forget_logit))
    length = column_of(length_ref[...]).astype(jnp.int32)
    length = jnp.concatenate([length, length], axis=0)
    gate = jnp.concatenate([gate_ref[:, 0, :], gate_ref[:, 1, :]], axis=0)
    entry = lax.broadcasted_iota(jnp.int32, (rows, cache_len), 1)
    last_gate = jnp.sum(jnp.where(entry == length - 1, gate, 0.0), axis=1, keepdims=True)
    current = last_gate + forget_log
    for copy in weight_copies:
        copy.wait()
    query, key_new, value_new = [
        jnp.dot(normed, wqkv[i], preferred_element_type=F32).astype(BF16).astype(F32)
        for i in range(3)
    ]
    lane = lax.broadcasted_iota(jnp.int32, (1, width), 1)
    first_head = lane < half
    own = query * key_new
    own_score = scale * jnp.concatenate(
        [
            jnp.sum(jnp.where(first_head, own, 0.0), axis=1, keepdims=True),
            jnp.sum(jnp.where(first_head, 0.0, own), axis=1, keepdims=True),
        ],
        axis=0,
    )
    row8 = lax.broadcasted_iota(jnp.int32, (8, width), 0)
    lane8 = lax.broadcasted_iota(jnp.int32, (8, width), 1)
    masks = [
        (row8 // heads == i) & ((lane8 < half) == (lax.rem(row8, heads) == 0)) for i in range(2)
    ]
    place_columns = routing_places(group_ref[...] * EXPERTS_PER_GROUP + slot_ref[...])
    combine_table(place_columns, route_weight_ref[...], table_ref)
    table_copy = pltpu.make_async_copy(table_ref, table_hbm, w_sems.at[4])
    table_copy.start()
    tail = jnp.zeros((seqs, width), F32)
    for k, place in enumerate(place_columns):
        tail = tail + jnp.where(lane == k, place.astype(F32), 0.0)
    tail = tail.astype(BF16)
    for g in range(seqs // key_group):
        key_copies[g].wait()
        for s in range(g * key_group, (g + 1) * key_group, 2):
            masked = jnp.concatenate(
                [jnp.where(masks[i], query[s + i : s + i + 1], 0.0) for i in range(2)], axis=1
            ).astype(BF16)
            pair = jnp.concatenate([keys[s], keys[s + 1]], axis=1)
            result = lax.dot_general(masked, pair, NT, preferred_element_type=F32)
            for i in range(2):
                for h in range(heads):
                    scores[h * seqs + s + i : h * seqs + s + i + 1] = result[
                        heads * i + h : heads * i + h + 1
                    ]
    score = scores[...] * scale + (current - gate)
    score = jnp.where(entry < length, score, -jnp.inf)
    peak = jnp.maximum(jnp.max(score, axis=1, keepdims=True), own_score)
    weights = jnp.exp(score - peak)
    own_weight = jnp.exp(own_score - peak)
    denominator = jnp.sum(weights, axis=1, keepdims=True) + own_weight
    scores[...] = weights
    for g in range(seqs // value_group):
        value_copies[g].wait()
        for s in range(g * value_group, (g + 1) * value_group, 2):
            four = jnp.concatenate(
                [
                    scores[h * seqs + s + i : h * seqs + s + i + 1]
                    for i in range(2)
                    for h in range(heads)
                ]
                + [jnp.zeros((4, cache_len), F32)],
                axis=0,
            ).astype(BF16)
            pair = jnp.concatenate([values[s], values[s + 1]], axis=1)
            result = jnp.dot(four, pair, preferred_element_type=F32)
            for i in range(2):
                mine = result[heads * i : heads * i + heads, i * width : (i + 1) * width]
                weighted[s + i : s + i + 1] = jnp.where(first_head, mine[0:1], mine[1:2])
    output_copy.wait()
    table_copy.wait()
    own_weight = own_weight.astype(BF16).astype(F32)
    own_weight = jnp.where(first_head, own_weight[:seqs], own_weight[seqs:])
    denominator = jnp.where(first_head, denominator[:seqs], denominator[seqs:])
    attended = ((weighted[...] + own_weight * value_new) / denominator).astype(BF16)
    head_part = jnp.dot(attended, wo[...], preferred_element_type=F32).astype(BF16)
    model_width = head_part.shape[1]
    for i in range(parts_ref.shape[0]):
        parts_ref[i, :, 0:model_width] = head_part
        parts_ref[i, :, model_width:] = tail


def column_of(row):
    n = row.shape[1]
    same = lax.broadcasted_iota(jnp.int32, (n, n), 0) == lax.broadcasted_iota(
        jnp.int32, (n, n), 1
    )
    return jnp.sum(jnp.where(same, row.astype(F32), 0.0), axis=1, keepdims=True)


def routing_places(ids):
    picks, seqs = ids.shape
    columns = [column_of(ids[k : k + 1]) for k in range(picks)]
    down = lax.broadcasted_iota(jnp.int32, (seqs, seqs), 0)
    across = lax.broadcasted_iota(jnp.int32, (seqs, seqs), 1)
    rows = [ids[k : k + 1].astype(F32) for k in range(picks)]
    places = []
    for column in columns:
        before = jnp.zeros((seqs, 1), F32)
        for row in rows:
            hit = (column == row) & (across < down)
            before = before + jnp.sum(jnp.where(hit, 1.0, 0.0), axis=1, keepdims=True)
        places.append((column * 8 + before).astype(jnp.int32))
    return places


def select_table(place_rows, position, rows):
    seqs = place_rows[0].shape[1]
    row = lax.broadcasted_iota(jnp.int32, (rows, 4 * seqs), 0)
    column = lax.broadcasted_iota(jnp.int32, (rows, 4 * seqs), 1)
    expert = row >> 3
    is_dense = (row & 1) == 1
    token = column & (seqs - 1)
    hit = is_dense & (token == position * 2 + (expert & 1))
    for place in place_rows:
        places = jnp.concatenate([place] * 4, axis=1)
        hit = hit | (jnp.logical_not(is_dense) & (places == expert * 8 + (position & 1)))
    same_quarter = ((row >> 1) & 3) == column // seqs
    return jnp.where(hit & same_quarter, 1.0, 0.0).astype(BF16)


def combine_table(place_columns, weight_rows, table_ref):
    seqs = place_columns[0].shape[0]
    wide = table_ref.shape[1]
    row = lax.broadcasted_iota(jnp.int32, (2 * seqs, wide), 0)
    column = lax.broadcasted_iota(jnp.int32, (2 * seqs, wide), 1)
    is_dense = (column & 1) == 1
    core = (column >> 1) & 1
    chip = (column >> 3) & 3
    expert = column >> 5
    same_half = ((column >> 2) & 1) == (row >= seqs).astype(jnp.int32)
    weight = jnp.zeros((2 * seqs, wide), F32)
    for k, place in enumerate(place_columns):
        places = jnp.concatenate([place, place], axis=0)
        value = column_of(weight_rows[k : k + 1])
        value = jnp.concatenate([value, value], axis=0)
        hit = same_half & jnp.logical_not(is_dense) & (places == expert * 8 + core)
        weight = weight + jnp.where(hit, value, 0.0)
    high = weight.astype(BF16)
    table_ref[0 : 2 * seqs] = high
    table_ref[2 * seqs : 4 * seqs] = (weight - high.astype(F32)).astype(BF16)
    dense = same_half & is_dense & ((row & (seqs - 1)) == chip * 4 + core * 2 + (expert & 1))
    table_ref[4 * seqs : 6 * seqs] = jnp.where(dense, 1.0, 0.0).astype(BF16)


def dispatch_kernel(
    position_ref,
    parts_ref,
    tokens_ref,
    gain_ref,
    mix_ref,
    out_ref,
    residual_ref,
    mix_gate_ref,
    scratch,
):
    quarter = out_ref.shape[1]
    width = residual_ref.shape[1]
    model_width = tokens_ref.shape[1]
    seqs = tokens_ref.shape[0]
    columns = parts_ref[0, :, model_width:].astype(F32)
    same = lax.broadcasted_iota(jnp.int32, (seqs, seqs), 0) == lax.broadcasted_iota(
        jnp.int32, (seqs, seqs), 1
    )
    place_rows = [
        jnp.sum(jnp.where(same, columns[:, k : k + 1], 0.0), axis=0, keepdims=True).astype(
            jnp.int32
        )
        for k in range(2)
    ]
    select = select_table(place_rows, position_ref[0], out_ref.shape[0])
    attn = parts_ref[0, :, 0:model_width].astype(F32)
    for i in range(1, parts_ref.shape[0]):
        attn = attn + parts_ref[i, :, 0:model_width].astype(F32)
    residual = tokens_ref[...].astype(F32) + attn
    scratch[...] = residual
    normed = rms_scale(residual, gain_ref[...]).astype(BF16)
    quarters = jnp.concatenate(
        [normed[:, q * quarter : (q + 1) * quarter] for q in range(4)], axis=0
    )
    mix_gate_ref[...] = jax.nn.sigmoid(
        jnp.sum(normed.astype(F32) * mix_ref[...], axis=1, keepdims=True)
    )
    mine = pl.ds(pl.multiple_of(position_ref[0] * width, width), width)
    residual_ref[...] = scratch[:, mine]
    out_ref[...] = jnp.dot(select, quarters, preferred_element_type=F32).astype(BF16)


def whole_rows(parts):
    rows, width = parts.shape
    parts = parts.reshape(rows // 8, 8, width)
    parts = parts + pltpu.roll(parts, 4, 1)
    return (parts + pltpu.roll(parts, 2, 1)).reshape(rows, width)


def mark_kernel(rows_hbm, mark_ref):
    mark_ref[...] = jnp.zeros_like(mark_ref)


LATE = (2, 3)


def expert_kernel(position_ref, own_ref, other_ref, gate_ref, up_ref, down_ref, *refs):
    keep_ref, send_ref, late, left, sems = refs[-5:]
    operands = refs[:-5]
    blocks = 2 * len(operands)
    copies = [
        pltpu.make_async_copy(operands[k], late.at[i], sems.at[i]) for i, k in enumerate(LATE)
    ]
    for copy in copies:
        copy.start()
    pairs = {k: operands[k] for k in range(len(operands)) if k not in LATE}
    pairs.update({k: late.at[i] for i, k in enumerate(LATE)})
    size = late.shape[1] // 2
    pieces = {
        2 * k + i: ref.at[pl.ds(i * size, size)] for k, ref in pairs.items() for i in range(2)
    }
    rows, quarter = own_ref.shape
    width = late.shape[2]
    kb = 4 * quarter // blocks
    position = position_ref[0]
    core = position & 1
    row = lax.broadcasted_iota(jnp.int32, (rows, 1), 0)
    for i, ref in enumerate((own_ref, other_ref)):
        values = ref[...].astype(F32)
        for q in range(4):
            mine = jnp.where(((row >> 1) & 3) == q, values, 0.0)
            left[i * rows : (i + 1) * rows, q * quarter : (q + 1) * quarter] = mine.astype(BF16)
    both = jnp.dot(
        left[...],
        jnp.concatenate([gate_ref[...], up_ref[...]], axis=1),
        preferred_element_type=F32,
    )
    both = whole_rows(both)
    row2 = lax.broadcasted_iota(jnp.int32, (2 * rows, 1), 0)
    is_dense = (row2 & 1) == 1
    picked = jnp.where(is_dense, 0.0, silu(both[:, :width]) * both[:, width:]).astype(BF16)
    both = None
    for k, piece in pieces.items():
        if k == 2 * LATE[0]:
            for copy in copies:
                copy.wait()
        inner = pl.ds(pl.multiple_of((position ^ k) * kb, kb), kb)
        weights = jnp.concatenate([piece[0:kb], piece[kb : 2 * kb]], axis=1)
        part = jnp.dot(left[:, inner], weights, preferred_element_type=F32)
        both = part if both is None else both + part
    both = whole_rows(both)
    hidden = jnp.where(is_dense, silu(both[:, :width]) * both[:, width:], 0.0).astype(BF16)
    hidden = jnp.concatenate([picked, hidden], axis=1)
    right = ((row >> 2) & 1) == 1
    is_own = ((row >> 1) & 1) == core
    for k, piece in pieces.items():
        t = position ^ k
        dense_down = jnp.concatenate(
            [piece[2 * kb : 2 * kb + width], piece[2 * kb + width : 2 * kb + 2 * width]], axis=1
        )
        whole = pl.ds(pl.multiple_of(t * kb, kb), kb)
        down = jnp.concatenate([down_ref[:, whole], dense_down], axis=0)
        result = jnp.dot(hidden, down, preferred_element_type=F32)
        result = jnp.where(is_own, result[:rows], result[rows:])
        result = jnp.where(right, result[:, width:], result[:, :width])
        result = result.reshape(rows // 8, 8, width)
        if k % 2 == 0:
            keep_ref[:, t >> 1] = result
        else:
            send_ref[:, t >> 1] = result.astype(BF16)


def add_kernel(keep_ref, got_ref, out_ref):
    out_ref[...] = (keep_ref[...] + got_ref[...].astype(F32)).astype(BF16)


def combine_kernel(rows_ref, table_ref, mix_ref, residual_ref, mark_ref, out_ref):
    seqs = mix_ref.shape[0]
    width = rows_ref.shape[1]
    sums = jnp.dot(table_ref[...], rows_ref[...], preferred_element_type=F32)
    mix = mix_ref[...]
    for p in range(2):
        picked = sums[p * seqs : (p + 1) * seqs] + sums[(2 + p) * seqs : (3 + p) * seqs]
        dense = sums[(4 + p) * seqs : (5 + p) * seqs]
        columns = slice(p * width, (p + 1) * width)
        out_ref[:, columns] = (residual_ref[:, columns] + picked + mix * dense).astype(BF16)


def limits(mib):
    return pltpu.CompilerParams(vmem_limit_bytes=mib * MIB)


def exchange(array, axis):
    return lax.all_to_all(array, axis, 0, 0, tiled=True)


def attention_call(*operands):
    tokens, key_cache = operands[0], operands[13]
    seqs, model_width = tokens.shape
    _, cache_len, head_width = key_cache.shape
    tp_count = 8
    return pl.pallas_call(
        attention_kernel,
        name="attention",
        out_shape=(
            jax.ShapeDtypeStruct((tp_count, seqs, model_width + head_width), BF16),
            jax.ShapeDtypeStruct((6 * seqs, EXPERTS * 4 * tp_count), BF16),
        ),
        in_specs=[ANY] * 15,
        out_specs=(VMEM, ANY),
        scratch_shapes=[
            pltpu.VMEM((seqs, model_width), BF16),
            pltpu.VMEM((1, model_width), F32),
            pltpu.VMEM((2, model_width), BF16),
            pltpu.VMEM((1, 2), F32),
            pltpu.VMEM((seqs, 2, cache_len), F32),
            pltpu.VMEM((1, seqs), jnp.int32),
            pltpu.VMEM((1, seqs), jnp.int32),
            pltpu.VMEM((2, seqs), jnp.int32),
            pltpu.VMEM((2, seqs), F32),
            pltpu.VMEM((6 * seqs, EXPERTS * 4 * tp_count), BF16),
            pltpu.VMEM((3, model_width, head_width), BF16),
            pltpu.VMEM((head_width, model_width), BF16),
            pltpu.VMEM((seqs, cache_len, head_width), BF16),
            pltpu.VMEM((seqs, cache_len, head_width), BF16),
            pltpu.VMEM((2 * seqs, cache_len), F32),
            pltpu.VMEM((seqs, head_width), F32),
            pltpu.SemaphoreType.DMA((9,)),
            pltpu.SemaphoreType.DMA((5,)),
            pltpu.SemaphoreType.DMA((16,)),
            pltpu.SemaphoreType.DMA((16,)),
        ],
        compiler_params=limits(60),
        cost_estimate=pl.CostEstimate(flops=10**9, bytes_accessed=12 * MIB, transcendentals=40000),
    )(*operands)


def body(
    tokens,
    norm_attn,
    w_query,
    w_key,
    w_value,
    w_forget,
    forget_bias,
    w_output,
    key_cache,
    value_cache,
    gate_cache,
    lengths,
    norm_ffn,
    route_group,
    route_slot,
    route_weight,
    expert_gate,
    expert_up,
    expert_down,
    dense_gate,
    dense_up,
    dense_down,
    mix_vector,
):
    seqs, model_width = tokens.shape
    ep_count = lax.axis_size(EP)
    tp_count = lax.axis_size(TP)
    tp_position = lax.axis_index(TP)
    width_local = model_width // tp_count
    head_width = key_cache.shape[2]

    own_dense = jnp.concatenate(
        [dense_gate, dense_up, dense_down[:, :head_width], dense_down[:, head_width:]], axis=0
    )
    ep_1 = lax.axis_size("ep_1")
    same, cross = [], []
    for e in range(ep_1):
        same += [(2 * e, 2 * e), (2 * e + 1, 2 * (e ^ 1) + 1)]
        cross += [(2 * e + 1, 2 * e), (2 * e, 2 * (e ^ 1) + 1)]
    first = []
    for route in (same, cross):
        first.append(lax.ppermute(own_dense, ("ep_1", "core"), route))
    pair = jnp.concatenate(first, axis=0)
    dense_weights = [pair]
    chips = lax.axis_size("y")
    for k in range(1, chips):
        dense_weights.append(lax.ppermute(pair, "y", [(i, i ^ k) for i in range(chips)]))
    sibling = [(0, 1), (1, 0)]
    parts, table = attention_call(
        tokens,
        norm_attn.reshape(1, -1),
        w_forget.T,
        forget_bias.reshape(1, -1),
        gate_cache,
        lengths.reshape(1, -1),
        route_group.reshape(1, -1),
        route_slot.T,
        route_weight.T,
        w_query,
        w_key,
        w_value,
        w_output,
        key_cache,
        value_cache,
    )
    parts = exchange(parts, TP)

    position = tp_position.reshape(1)
    row_count = ep_count * 8
    wide = row_count * tp_count // 2
    dispatch = pl.pallas_call(
        dispatch_kernel,
        name="dispatch",
        out_shape=(
            jax.ShapeDtypeStruct((row_count, model_width // 4), BF16),
            jax.ShapeDtypeStruct((seqs, width_local), F32),
            jax.ShapeDtypeStruct((seqs, 1), F32),
        ),
        in_specs=[SMEM] + [VMEM] * 4,
        out_specs=(VMEM, VMEM, VMEM),
        scratch_shapes=[pltpu.VMEM((seqs, model_width), F32)],
        compiler_params=limits(8),
    )
    outgoing, residual, mix_gate = dispatch(
        position,
        parts,
        tokens,
        norm_ffn.reshape(1, -1),
        mix_vector.reshape(1, -1),
    )
    arrived = exchange(outgoing.reshape(ep_count, 8, -1), EP).reshape(row_count, -1)
    mark = pl.pallas_call(
        mark_kernel,
        name="mark",
        out_shape=jax.ShapeDtypeStruct((8, 128), F32),
        in_specs=[ANY],
        out_specs=VMEM,
        compiler_params=limits(8),
    )(arrived)
    other = lax.ppermute(arrived, "core", sibling)
    blocks = (ep_count, tp_count // 2, 8, width_local // 2)
    keep, send = pl.pallas_call(
        expert_kernel,
        name="experts",
        out_shape=(jax.ShapeDtypeStruct(blocks, F32), jax.ShapeDtypeStruct(blocks, BF16)),
        in_specs=[SMEM] + [VMEM] * 5 + [ANY if k in LATE else VMEM for k in range(chips)],
        out_specs=(VMEM, VMEM),
        scratch_shapes=[
            pltpu.VMEM((len(LATE), *pair.shape), BF16),
            pltpu.VMEM((2 * row_count, model_width), BF16),
            pltpu.SemaphoreType.DMA((len(LATE),)),
        ],
        compiler_params=limits(16),
    )(position, arrived, other, expert_gate[0], expert_up[0], expert_down[0], *dense_weights)
    got = lax.ppermute(send, "core", sibling)
    results = pl.pallas_call(
        add_kernel,
        name="add",
        out_shape=jax.ShapeDtypeStruct(blocks, BF16),
        in_specs=[VMEM] * 2,
        out_specs=VMEM,
        compiler_params=limits(8),
    )(keep, got)
    returned = exchange(
        results.reshape(ep_count * tp_count // 2, 8, width_local // 2), (*EP, "y")
    ).reshape(wide, width_local // 2)
    return pl.pallas_call(
        combine_kernel,
        name="combine",
        out_shape=jax.ShapeDtypeStruct((seqs, width_local), BF16),
        in_specs=[VMEM] * 4 + [ANY],
        out_specs=VMEM,
        compiler_params=limits(8),
    )(returned, table, mix_gate, residual, mark)


def solution(mesh):
    split = Mesh(mesh.devices.reshape(8, 4, 4, 2), ("ep_0", "ep_1", "y", "core"))
    return jax.shard_map(
        body,
        mesh=split,
        in_specs=(
            P(EP, None),
            P(),
            P(None, TP),
            P(None, TP),
            P(None, TP),
            P(None, TP),
            P(TP),
            P(TP, None),
            P(EP, None, TP),
            P(EP, None, TP),
            P(EP, TP, None),
            P(EP),
            P(),
            P(EP),
            P(EP, None),
            P(EP, None),
            P(EP, None, TP),
            P(EP, None, TP),
            P(EP, TP, None),
            P(TP, EP),
            P(TP, EP),
            P(EP, TP),
            P(),
        ),
        out_specs=P(EP, TP),
        check_vma=False,
    )
```

```python
import jax
import jax.numpy as jnp
from jax import lax
from jax.experimental import pallas as pl
from jax.experimental.pallas import tpu as pltpu
from jax.sharding import Mesh
from jax.sharding import PartitionSpec as P

EXPERTS_PER_GROUP = 8
EXPERTS = 32
EP = ("ep_0", "ep_1")
TP = ("y", "core")
EPS = 1e-06
F32 = jnp.float32
BF16 = jnp.bfloat16
NT = (((1,), (1,)), ((), ()))
VMEM = pl.BlockSpec(memory_space=pltpu.VMEM)
SMEM = pl.BlockSpec(memory_space=pltpu.SMEM)
ANY = pl.BlockSpec(memory_space=pl.ANY)
MIB = 1 << 20


def rms_scale(rows, gain):
    rows = rows.astype(F32)
    return rows * lax.rsqrt(jnp.mean(rows * rows, axis=-1, keepdims=True) + EPS) * gain


def silu(v):
    return v * jax.nn.sigmoid(v)


def stacked(pair):
    return jnp.concatenate([pair[:, 0:1], pair[:, 1:2]], axis=0)


def attention_kernel(
    tokens_hbm,
    gain_hbm,
    forget_hbm,
    bias_hbm,
    gate_hbm,
    length_hbm,
    group_hbm,
    slot_hbm,
    route_weight_hbm,
    wq_hbm,
    wk_hbm,
    wv_hbm,
    wo_hbm,
    key_hbm,
    value_hbm,
    parts_ref,
    table_hbm,
    tokens_ref,
    gain_ref,
    forget_ref,
    bias_ref,
    gate_ref,
    length_ref,
    group_ref,
    slot_ref,
    route_weight_ref,
    table_ref,
    wqkv,
    wo,
    keys,
    values,
    scores,
    weighted,
    small_sems,
    w_sems,
    key_sems,
    value_sems,
):
    seqs, cache_len, width = keys.shape
    heads = 2
    half = width // heads
    rows = heads * seqs
    scale = half ** (-0.5)
    key_group, value_group = 16, 16
    small = [
        pltpu.make_async_copy(src, dst, small_sems.at[i])
        for i, (src, dst) in enumerate(
            (
                (tokens_hbm, tokens_ref),
                (gain_hbm, gain_ref),
                (forget_hbm, forget_ref),
                (bias_hbm, bias_ref),
                (length_hbm, length_ref),
                (gate_hbm, gate_ref),
                (group_hbm, group_ref),
                (slot_hbm, slot_ref),
                (route_weight_hbm, route_weight_ref),
            )
        )
    ]
    weight_copies = [
        pltpu.make_async_copy(src, wqkv.at[i], w_sems.at[i])
        for i, src in enumerate((wq_hbm, wk_hbm, wv_hbm))
    ]
    output_copy = pltpu.make_async_copy(wo_hbm, wo, w_sems.at[3])
    part = lambda g, n: pl.ds(g * n, n)
    key_copies = [
        pltpu.make_async_copy(key_hbm.at[part(g, key_group)], keys.at[part(g, key_group)], key_sems.at[g])
        for g in range(seqs // key_group)
    ]
    value_copies = [
        pltpu.make_async_copy(value_hbm.at[part(g, value_group)], values.at[part(g, value_group)], value_sems.at[g])
        for g in range(seqs // value_group)
    ]
    for copy in small + weight_copies + key_copies + value_copies + [output_copy]:
        copy.start()
    for copy in small:
        copy.wait()
    normed = rms_scale(tokens_ref[...], gain_ref[...]).astype(BF16)
    forget_logit = (
        lax.dot_general(normed, forget_ref[...], NT, preferred_element_type=F32) + bias_ref[...]
    )
    forget_log = stacked(jax.nn.log_sigmoid(forget_logit))
    length = column_of(length_ref[...]).astype(jnp.int32)
    length = jnp.concatenate([length, length], axis=0)
    gate = jnp.concatenate([gate_ref[:, 0, :], gate_ref[:, 1, :]], axis=0)
    entry = lax.broadcasted_iota(jnp.int32, (rows, cache_len), 1)
    last_gate = jnp.sum(jnp.where(entry == length - 1, gate, 0.0), axis=1, keepdims=True)
    current = last_gate + forget_log
    for copy in weight_copies:
        copy.wait()
    query, key_new, value_new = [
        jnp.dot(normed, wqkv[i], preferred_element_type=F32).astype(BF16).astype(F32)
        for i in range(3)
    ]
    lane = lax.broadcasted_iota(jnp.int32, (1, width), 1)
    first_head = lane < half
    own = query * key_new
    own_score = scale * jnp.concatenate(
        [
            jnp.sum(jnp.where(first_head, own, 0.0), axis=1, keepdims=True),
            jnp.sum(jnp.where(first_head, 0.0, own), axis=1, keepdims=True),
        ],
        axis=0,
    )
    row8 = lax.broadcasted_iota(jnp.int32, (8, width), 0)
    lane8 = lax.broadcasted_iota(jnp.int32, (8, width), 1)
    masks = [
        (row8 // heads == i) & ((lane8 < half) == (lax.rem(row8, heads) == 0)) for i in range(2)
    ]
    place_columns = routing_places(group_ref[...] * EXPERTS_PER_GROUP + slot_ref[...])
    combine_table(place_columns, route_weight_ref[...], table_ref)
    table_copy = pltpu.make_async_copy(table_ref, table_hbm, w_sems.at[4])
    table_copy.start()
    tail = jnp.zeros((seqs, width), F32)
    for k, place in enumerate(place_columns):
        tail = tail + jnp.where(lane == k, place.astype(F32), 0.0)
    tail = tail.astype(BF16)
    for g in range(seqs // key_group):
        key_copies[g].wait()
        for s in range(g * key_group, (g + 1) * key_group, 2):
            masked = jnp.concatenate(
                [jnp.where(masks[i], query[s + i : s + i + 1], 0.0) for i in range(2)], axis=1
            ).astype(BF16)
            pair = jnp.concatenate([keys[s], keys[s + 1]], axis=1)
            result = lax.dot_general(masked, pair, NT, preferred_element_type=F32)
            for i in range(2):
                for h in range(heads):
                    scores[h * seqs + s + i : h * seqs + s + i + 1] = result[
                        heads * i + h : heads * i + h + 1
                    ]
    score = scores[...] * scale + (current - gate)
    score = jnp.where(entry < length, score, -jnp.inf)
    peak = jnp.maximum(jnp.max(score, axis=1, keepdims=True), own_score)
    weights = jnp.exp(score - peak)
    own_weight = jnp.exp(own_score - peak)
    denominator = jnp.sum(weights, axis=1, keepdims=True) + own_weight
    scores[...] = weights
    for g in range(seqs // value_group):
        value_copies[g].wait()
        for s in range(g * value_group, (g + 1) * value_group, 2):
            four = jnp.concatenate(
                [
                    scores[h * seqs + s + i : h * seqs + s + i + 1]
                    for i in range(2)
                    for h in range(heads)
                ]
                + [jnp.zeros((4, cache_len), F32)],
                axis=0,
            ).astype(BF16)
            pair = jnp.concatenate([values[s], values[s + 1]], axis=1)
            result = jnp.dot(four, pair, preferred_element_type=F32)
            for i in range(2):
                mine = result[heads * i : heads * i + heads, i * width : (i + 1) * width]
                weighted[s + i : s + i + 1] = jnp.where(first_head, mine[0:1], mine[1:2])
    output_copy.wait()
    table_copy.wait()
    own_weight = own_weight.astype(BF16).astype(F32)
    own_weight = jnp.where(first_head, own_weight[:seqs], own_weight[seqs:])
    denominator = jnp.where(first_head, denominator[:seqs], denominator[seqs:])
    attended = ((weighted[...] + own_weight * value_new) / denominator).astype(BF16)
    head_part = jnp.dot(attended, wo[...], preferred_element_type=F32).astype(BF16)
    model_width = head_part.shape[1]
    for i in range(parts_ref.shape[0]):
        parts_ref[i, :, 0:model_width] = head_part
        parts_ref[i, :, model_width:] = tail


def column_of(row):
    n = row.shape[1]
    same = lax.broadcasted_iota(jnp.int32, (n, n), 0) == lax.broadcasted_iota(
        jnp.int32, (n, n), 1
    )
    return jnp.sum(jnp.where(same, row.astype(F32), 0.0), axis=1, keepdims=True)


def routing_places(ids):
    picks, seqs = ids.shape
    columns = [column_of(ids[k : k + 1]) for k in range(picks)]
    down = lax.broadcasted_iota(jnp.int32, (seqs, seqs), 0)
    across = lax.broadcasted_iota(jnp.int32, (seqs, seqs), 1)
    rows = [ids[k : k + 1].astype(F32) for k in range(picks)]
    places = []
    for column in columns:
        before = jnp.zeros((seqs, 1), F32)
        for row in rows:
            hit = (column == row) & (across < down)
            before = before + jnp.sum(jnp.where(hit, 1.0, 0.0), axis=1, keepdims=True)
        places.append((column * 8 + before).astype(jnp.int32))
    return places


def select_table(place_rows, position, rows):
    seqs = place_rows[0].shape[1]
    row = lax.broadcasted_iota(jnp.int32, (rows, 4 * seqs), 0)
    column = lax.broadcasted_iota(jnp.int32, (rows, 4 * seqs), 1)
    expert = row >> 3
    is_dense = (row & 1) == 1
    token = column & (seqs - 1)
    hit = is_dense & (token == position * 2 + (expert & 1))
    for place in place_rows:
        places = jnp.concatenate([place] * 4, axis=1)
        hit = hit | (jnp.logical_not(is_dense) & (places == expert * 8 + (position & 1)))
    same_quarter = ((row >> 1) & 3) == column // seqs
    return jnp.where(hit & same_quarter, 1.0, 0.0).astype(BF16)


def combine_table(place_columns, weight_rows, table_ref):
    seqs = place_columns[0].shape[0]
    wide = table_ref.shape[1]
    row = lax.broadcasted_iota(jnp.int32, (2 * seqs, wide), 0)
    column = lax.broadcasted_iota(jnp.int32, (2 * seqs, wide), 1)
    is_dense = (column & 1) == 1
    core = (column >> 1) & 1
    chip = (column >> 3) & 3
    expert = column >> 5
    same_half = ((column >> 2) & 1) == (row >= seqs).astype(jnp.int32)
    weight = jnp.zeros((2 * seqs, wide), F32)
    for k, place in enumerate(place_columns):
        places = jnp.concatenate([place, place], axis=0)
        value = column_of(weight_rows[k : k + 1])
        value = jnp.concatenate([value, value], axis=0)
        hit = same_half & jnp.logical_not(is_dense) & (places == expert * 8 + core)
        weight = weight + jnp.where(hit, value, 0.0)
    high = weight.astype(BF16)
    table_ref[0 : 2 * seqs] = high
    table_ref[2 * seqs : 4 * seqs] = (weight - high.astype(F32)).astype(BF16)
    dense = same_half & is_dense & ((row & (seqs - 1)) == chip * 4 + core * 2 + (expert & 1))
    table_ref[4 * seqs : 6 * seqs] = jnp.where(dense, 1.0, 0.0).astype(BF16)


def dispatch_kernel(
    position_ref,
    parts_ref,
    tokens_ref,
    gain_ref,
    mix_ref,
    out_ref,
    residual_ref,
    mix_gate_ref,
    scratch,
):
    quarter = out_ref.shape[1]
    width = residual_ref.shape[1]
    model_width = tokens_ref.shape[1]
    seqs = tokens_ref.shape[0]
    columns = parts_ref[0, :, model_width:].astype(F32)
    same = lax.broadcasted_iota(jnp.int32, (seqs, seqs), 0) == lax.broadcasted_iota(
        jnp.int32, (seqs, seqs), 1
    )
    place_rows = [
        jnp.sum(jnp.where(same, columns[:, k : k + 1], 0.0), axis=0, keepdims=True).astype(
            jnp.int32
        )
        for k in range(2)
    ]
    select = select_table(place_rows, position_ref[0], out_ref.shape[0])
    attn = parts_ref[0, :, 0:model_width].astype(F32)
    for i in range(1, parts_ref.shape[0]):
        attn = attn + parts_ref[i, :, 0:model_width].astype(F32)
    residual = tokens_ref[...].astype(F32) + attn
    scratch[...] = residual
    normed = rms_scale(residual, gain_ref[...]).astype(BF16)
    quarters = jnp.concatenate(
        [normed[:, q * quarter : (q + 1) * quarter] for q in range(4)], axis=0
    )
    mix_gate_ref[...] = jax.nn.sigmoid(
        jnp.sum(normed.astype(F32) * mix_ref[...], axis=1, keepdims=True)
    )
    mine = pl.ds(pl.multiple_of(position_ref[0] * width, width), width)
    residual_ref[...] = scratch[:, mine]
    out_ref[...] = jnp.dot(select, quarters, preferred_element_type=F32).astype(BF16)


def whole_rows(parts):
    rows, width = parts.shape
    parts = parts.reshape(rows // 8, 8, width)
    parts = parts + pltpu.roll(parts, 4, 1)
    return (parts + pltpu.roll(parts, 2, 1)).reshape(rows, width)


def spread(values, out_ref, start):
    rows, quarter = values.shape
    values = values.astype(F32)
    row = lax.broadcasted_iota(jnp.int32, (rows, 1), 0)
    for q in range(4):
        mine = jnp.where(((row >> 1) & 3) == q, values, 0.0)
        out_ref[start : start + rows, q * quarter : (q + 1) * quarter] = mine.astype(BF16)


def picked_hidden(left, gate_ref, up_ref):
    width = gate_ref.shape[1]
    weights = jnp.concatenate([gate_ref[...], up_ref[...]], axis=1)
    both = whole_rows(jnp.dot(left, weights, preferred_element_type=F32))
    row = lax.broadcasted_iota(jnp.int32, (both.shape[0], 1), 0)
    hidden = silu(both[:, :width]) * both[:, width:]
    return jnp.where((row & 1) == 1, 0.0, hidden).astype(BF16)


def own_kernel(own_ref, gate_ref, up_ref, left_ref, picked_ref):
    spread(own_ref[...], left_ref, 0)
    picked_ref[...] = picked_hidden(left_ref[...], gate_ref, up_ref)


LATE = (1, 2)


def split_pairs(operands):
    size = operands[0].shape[0] // 2
    return {
        2 * k + i: operands[k].at[pl.ds(i * size, size)]
        for k in sorted(range(len(operands)), key=LATE.count)
        for i in range(2)
    }


def down_block(position, k, hidden, down_ref, piece, rows):
    width = piece.shape[1]
    kb = 2 * width
    row = lax.broadcasted_iota(jnp.int32, (rows, 1), 0)
    right = ((row >> 2) & 1) == 1
    is_own = ((row >> 1) & 1) == (position & 1)
    dense_down = jnp.concatenate(
        [piece[2 * kb : 2 * kb + width], piece[2 * kb + width : 2 * kb + 2 * width]], axis=1
    )
    whole = pl.ds(pl.multiple_of((position ^ k) * kb, kb), kb)
    down = jnp.concatenate([down_ref[:, whole], dense_down], axis=0)
    result = jnp.dot(hidden, down, preferred_element_type=F32)
    result = jnp.where(is_own, result[:rows], result[rows:])
    result = jnp.where(right, result[:, width:], result[:, :width])
    return result.reshape(rows // 8, 8, width)


def expert_kernel(
    position_ref, left_ref, picked_ref, other_ref, gate_ref, up_ref, down_ref, *refs
):
    send_ref, hidden_ref, late, left, sems = refs[-5:]
    operands = list(refs[:-5])
    copies = [
        pltpu.make_async_copy(operands[k], late.at[i], sems.at[i]) for i, k in enumerate(LATE)
    ]
    for copy in copies:
        copy.start()
    for i, k in enumerate(LATE):
        operands[k] = late.at[i]
    pieces = split_pairs(operands)
    rows = other_ref.shape[0]
    width = late.shape[2]
    kb = 2 * width
    position = position_ref[0]
    spread(other_ref[...], left, 0)
    picked = picked_hidden(left[...], gate_ref, up_ref)
    sums = [None, None]
    for k, piece in pieces.items():
        if k == 2 * LATE[0]:
            for copy in copies:
                copy.wait()
        inner = pl.ds(pl.multiple_of((position ^ k) * kb, kb), kb)
        weights = jnp.concatenate([piece[0:kb], piece[kb : 2 * kb]], axis=1)
        for i, ref in enumerate((left_ref, left)):
            part = jnp.dot(ref[:, inner], weights, preferred_element_type=F32)
            sums[i] = part if sums[i] is None else sums[i] + part
    row = lax.broadcasted_iota(jnp.int32, (rows, 1), 0)
    for i, known in enumerate((picked_ref[...], picked)):
        both = whole_rows(sums[i])
        dense = silu(both[:, :width]) * both[:, width:]
        dense = jnp.where((row & 1) == 1, dense, 0.0).astype(BF16)
        hidden_ref[i * rows : (i + 1) * rows] = jnp.concatenate([known, dense], axis=1)
    hidden = hidden_ref[...]
    for k, piece in pieces.items():
        if k % 2 == 1:
            block = down_block(position, k, hidden, down_ref, piece, rows)
            send_ref[:, (position ^ k) >> 1] = block.astype(BF16)


def keep_kernel(position_ref, hidden_ref, down_ref, *refs):
    keep_ref = refs[-1]
    position = position_ref[0]
    hidden = hidden_ref[...]
    rows = hidden.shape[0] // 2
    for k, piece in split_pairs(refs[:-1]).items():
        if k % 2 == 0:
            block = down_block(position, k, hidden, down_ref, piece, rows)
            keep_ref[:, (position ^ k) >> 1] = block


def add_kernel(keep_ref, got_ref, out_ref):
    out_ref[...] = (keep_ref[...] + got_ref[...].astype(F32)).astype(BF16)


def combine_kernel(rows_ref, table_ref, mix_ref, residual_ref, out_ref):
    seqs = mix_ref.shape[0]
    width = rows_ref.shape[1]
    sums = jnp.dot(table_ref[...], rows_ref[...], preferred_element_type=F32)
    mix = mix_ref[...]
    for p in range(2):
        picked = sums[p * seqs : (p + 1) * seqs] + sums[(2 + p) * seqs : (3 + p) * seqs]
        dense = sums[(4 + p) * seqs : (5 + p) * seqs]
        columns = slice(p * width, (p + 1) * width)
        out_ref[:, columns] = (residual_ref[:, columns] + picked + mix * dense).astype(BF16)


def limits(mib):
    return pltpu.CompilerParams(vmem_limit_bytes=mib * MIB)


def exchange(array, axis):
    return lax.all_to_all(array, axis, 0, 0, tiled=True)


def attention_call(*operands):
    tokens, key_cache = operands[0], operands[13]
    seqs, model_width = tokens.shape
    _, cache_len, head_width = key_cache.shape
    tp_count = 8
    return pl.pallas_call(
        attention_kernel,
        name="attention",
        out_shape=(
            jax.ShapeDtypeStruct((tp_count, seqs, model_width + head_width), BF16),
            jax.ShapeDtypeStruct((6 * seqs, EXPERTS * 4 * tp_count), BF16),
        ),
        in_specs=[ANY] * 15,
        out_specs=(VMEM, ANY),
        scratch_shapes=[
            pltpu.VMEM((seqs, model_width), BF16),
            pltpu.VMEM((1, model_width), F32),
            pltpu.VMEM((2, model_width), BF16),
            pltpu.VMEM((1, 2), F32),
            pltpu.VMEM((seqs, 2, cache_len), F32),
            pltpu.VMEM((1, seqs), jnp.int32),
            pltpu.VMEM((1, seqs), jnp.int32),
            pltpu.VMEM((2, seqs), jnp.int32),
            pltpu.VMEM((2, seqs), F32),
            pltpu.VMEM((6 * seqs, EXPERTS * 4 * tp_count), BF16),
            pltpu.VMEM((3, model_width, head_width), BF16),
            pltpu.VMEM((head_width, model_width), BF16),
            pltpu.VMEM((seqs, cache_len, head_width), BF16),
            pltpu.VMEM((seqs, cache_len, head_width), BF16),
            pltpu.VMEM((2 * seqs, cache_len), F32),
            pltpu.VMEM((seqs, head_width), F32),
            pltpu.SemaphoreType.DMA((9,)),
            pltpu.SemaphoreType.DMA((5,)),
            pltpu.SemaphoreType.DMA((16,)),
            pltpu.SemaphoreType.DMA((16,)),
        ],
        compiler_params=limits(60),
        cost_estimate=pl.CostEstimate(flops=10**9, bytes_accessed=12 * MIB, transcendentals=40000),
    )(*operands)


def body(
    tokens,
    norm_attn,
    w_query,
    w_key,
    w_value,
    w_forget,
    forget_bias,
    w_output,
    key_cache,
    value_cache,
    gate_cache,
    lengths,
    norm_ffn,
    route_group,
    route_slot,
    route_weight,
    expert_gate,
    expert_up,
    expert_down,
    dense_gate,
    dense_up,
    dense_down,
    mix_vector,
):
    seqs, model_width = tokens.shape
    ep_count = lax.axis_size(EP)
    tp_count = lax.axis_size(TP)
    tp_position = lax.axis_index(TP)
    width_local = model_width // tp_count
    head_width = key_cache.shape[2]

    own_dense = jnp.concatenate(
        [dense_gate, dense_up, dense_down[:, :head_width], dense_down[:, head_width:]], axis=0
    )
    ep_1 = lax.axis_size("ep_1")
    same, cross = [], []
    for e in range(ep_1):
        same += [(2 * e, 2 * e), (2 * e + 1, 2 * (e ^ 1) + 1)]
        cross += [(2 * e + 1, 2 * e), (2 * e, 2 * (e ^ 1) + 1)]
    first = []
    for route in (same, cross):
        first.append(lax.ppermute(own_dense, ("ep_1", "core"), route))
    pair = jnp.concatenate(first, axis=0)
    dense_weights = [pair]
    chips = lax.axis_size("y")
    for k in range(1, chips):
        dense_weights.append(lax.ppermute(pair, "y", [(i, i ^ k) for i in range(chips)]))
    sibling = [(0, 1), (1, 0)]
    parts, table = attention_call(
        tokens,
        norm_attn.reshape(1, -1),
        w_forget.T,
        forget_bias.reshape(1, -1),
        gate_cache,
        lengths.reshape(1, -1),
        route_group.reshape(1, -1),
        route_slot.T,
        route_weight.T,
        w_query,
        w_key,
        w_value,
        w_output,
        key_cache,
        value_cache,
    )
    parts = exchange(parts, TP)

    position = tp_position.reshape(1)
    row_count = ep_count * 8
    wide = row_count * tp_count // 2
    dispatch = pl.pallas_call(
        dispatch_kernel,
        name="dispatch",
        out_shape=(
            jax.ShapeDtypeStruct((row_count, model_width // 4), BF16),
            jax.ShapeDtypeStruct((seqs, width_local), F32),
            jax.ShapeDtypeStruct((seqs, 1), F32),
        ),
        in_specs=[SMEM] + [VMEM] * 4,
        out_specs=(VMEM, VMEM, VMEM),
        scratch_shapes=[pltpu.VMEM((seqs, model_width), F32)],
        compiler_params=limits(8),
    )
    outgoing, residual, mix_gate = dispatch(
        position,
        parts,
        tokens,
        norm_ffn.reshape(1, -1),
        mix_vector.reshape(1, -1),
    )
    arrived = exchange(outgoing.reshape(ep_count, 8, -1), EP).reshape(row_count, -1)
    other = lax.ppermute(arrived, "core", sibling)
    left, picked = pl.pallas_call(
        own_kernel,
        name="own",
        out_shape=(
            jax.ShapeDtypeStruct((row_count, model_width), BF16),
            jax.ShapeDtypeStruct((row_count, head_width), BF16),
        ),
        in_specs=[VMEM] * 3,
        out_specs=(VMEM, VMEM),
        compiler_params=limits(8),
    )(arrived, expert_gate[0], expert_up[0])
    blocks = (ep_count, tp_count // 2, 8, width_local // 2)
    send, hidden = pl.pallas_call(
        expert_kernel,
        name="experts",
        out_shape=(
            jax.ShapeDtypeStruct(blocks, BF16),
            jax.ShapeDtypeStruct((2 * row_count, 2 * head_width), BF16),
        ),
        in_specs=[SMEM] + [VMEM] * 6 + [ANY if k in LATE else VMEM for k in range(chips)],
        out_specs=(VMEM, VMEM),
        scratch_shapes=[
            pltpu.VMEM((len(LATE), *pair.shape), BF16),
            pltpu.VMEM((row_count, model_width), BF16),
            pltpu.SemaphoreType.DMA((len(LATE),)),
        ],
        compiler_params=limits(16),
    )(
        position,
        left,
        picked,
        other,
        expert_gate[0],
        expert_up[0],
        expert_down[0],
        *dense_weights,
    )
    got = lax.ppermute(send, "core", sibling)
    keep = pl.pallas_call(
        keep_kernel,
        name="keep",
        out_shape=jax.ShapeDtypeStruct(blocks, F32),
        in_specs=[SMEM] + [VMEM] * (2 + chips),
        out_specs=VMEM,
        compiler_params=limits(8),
    )(position, hidden, expert_down[0], *dense_weights)
    results = pl.pallas_call(
        add_kernel,
        name="add",
        out_shape=jax.ShapeDtypeStruct(blocks, BF16),
        in_specs=[VMEM] * 2,
        out_specs=VMEM,
        compiler_params=limits(8),
    )(keep, got)
    returned = exchange(
        results.reshape(ep_count * tp_count // 2, 8, width_local // 2), (*EP, "y")
    ).reshape(wide, width_local // 2)
    return pl.pallas_call(
        combine_kernel,
        name="combine",
        out_shape=jax.ShapeDtypeStruct((seqs, width_local), BF16),
        in_specs=[VMEM] * 4,
        out_specs=VMEM,
        compiler_params=limits(8),
    )(returned, table, mix_gate, residual)


def solution(mesh):
    split = Mesh(mesh.devices.reshape(8, 4, 4, 2), ("ep_0", "ep_1", "y", "core"))
    return jax.shard_map(
        body,
        mesh=split,
        in_specs=(
            P(EP, None),
            P(),
            P(None, TP),
            P(None, TP),
            P(None, TP),
            P(None, TP),
            P(TP),
            P(TP, None),
            P(EP, None, TP),
            P(EP, None, TP),
            P(EP, TP, None),
            P(EP),
            P(),
            P(EP),
            P(EP, None),
            P(EP, None),
            P(EP, None, TP),
            P(EP, None, TP),
            P(EP, TP, None),
            P(TP, EP),
            P(TP, EP),
            P(EP, TP),
            P(),
        ),
        out_specs=P(EP, TP),
        check_vma=False,
    )
```

```python
import jax
import jax.numpy as jnp
from jax import lax
from jax.experimental import pallas as pl
from jax.experimental.pallas import tpu as pltpu
from jax.sharding import Mesh
from jax.sharding import PartitionSpec as P

EXPERTS_PER_GROUP = 8
EXPERTS = 32
EP = ("ep_0", "ep_1")
TP = ("y", "core")
EPS = 1e-06
F32 = jnp.float32
BF16 = jnp.bfloat16
NT = (((1,), (1,)), ((), ()))
VMEM = pl.BlockSpec(memory_space=pltpu.VMEM)
SMEM = pl.BlockSpec(memory_space=pltpu.SMEM)
ANY = pl.BlockSpec(memory_space=pl.ANY)
MIB = 1 << 20


def rms_scale(rows, gain):
    rows = rows.astype(F32)
    return rows * lax.rsqrt(jnp.mean(rows * rows, axis=-1, keepdims=True) + EPS) * gain


def silu(v):
    return v * jax.nn.sigmoid(v)


def stacked(pair):
    return jnp.concatenate([pair[:, 0:1], pair[:, 1:2]], axis=0)


def attention_kernel(
    tokens_hbm,
    gain_hbm,
    forget_hbm,
    bias_hbm,
    gate_hbm,
    length_hbm,
    group_hbm,
    slot_hbm,
    route_weight_hbm,
    wq_hbm,
    wk_hbm,
    wv_hbm,
    wo_hbm,
    key_hbm,
    value_hbm,
    parts_ref,
    table_hbm,
    tokens_ref,
    gain_ref,
    forget_ref,
    bias_ref,
    gate_ref,
    length_ref,
    group_ref,
    slot_ref,
    route_weight_ref,
    table_ref,
    wqkv,
    wo,
    keys,
    values,
    scores,
    weighted,
    small_sems,
    w_sems,
    key_sems,
    value_sems,
):
    seqs, cache_len, width = keys.shape
    heads = 2
    half = width // heads
    rows = heads * seqs
    scale = half ** (-0.5)
    key_group, value_group = 16, 16
    small = [
        pltpu.make_async_copy(src, dst, small_sems.at[i])
        for i, (src, dst) in enumerate(
            (
                (tokens_hbm, tokens_ref),
                (gain_hbm, gain_ref),
                (forget_hbm, forget_ref),
                (bias_hbm, bias_ref),
                (length_hbm, length_ref),
                (gate_hbm, gate_ref),
                (group_hbm, group_ref),
                (slot_hbm, slot_ref),
                (route_weight_hbm, route_weight_ref),
            )
        )
    ]
    weight_copies = [
        pltpu.make_async_copy(src, wqkv.at[i], w_sems.at[i])
        for i, src in enumerate((wq_hbm, wk_hbm, wv_hbm))
    ]
    output_copy = pltpu.make_async_copy(wo_hbm, wo, w_sems.at[3])
    part = lambda g, n: pl.ds(g * n, n)
    key_copies = [
        pltpu.make_async_copy(key_hbm.at[part(g, key_group)], keys.at[part(g, key_group)], key_sems.at[g])
        for g in range(seqs // key_group)
    ]
    value_copies = [
        pltpu.make_async_copy(value_hbm.at[part(g, value_group)], values.at[part(g, value_group)], value_sems.at[g])
        for g in range(seqs // value_group)
    ]
    for copy in small + weight_copies + key_copies + value_copies + [output_copy]:
        copy.start()
    for copy in small:
        copy.wait()
    normed = rms_scale(tokens_ref[...], gain_ref[...]).astype(BF16)
    forget_logit = (
        lax.dot_general(normed, forget_ref[...], NT, preferred_element_type=F32) + bias_ref[...]
    )
    forget_log = stacked(jax.nn.log_sigmoid(forget_logit))
    length = column_of(length_ref[...]).astype(jnp.int32)
    length = jnp.concatenate([length, length], axis=0)
    gate = jnp.concatenate([gate_ref[:, 0, :], gate_ref[:, 1, :]], axis=0)
    entry = lax.broadcasted_iota(jnp.int32, (rows, cache_len), 1)
    last_gate = jnp.sum(jnp.where(entry == length - 1, gate, 0.0), axis=1, keepdims=True)
    current = last_gate + forget_log
    for copy in weight_copies:
        copy.wait()
    query, key_new, value_new = [
        jnp.dot(normed, wqkv[i], preferred_element_type=F32).astype(BF16).astype(F32)
        for i in range(3)
    ]
    lane = lax.broadcasted_iota(jnp.int32, (1, width), 1)
    first_head = lane < half
    own = query * key_new
    own_score = scale * jnp.concatenate(
        [
            jnp.sum(jnp.where(first_head, own, 0.0), axis=1, keepdims=True),
            jnp.sum(jnp.where(first_head, 0.0, own), axis=1, keepdims=True),
        ],
        axis=0,
    )
    row8 = lax.broadcasted_iota(jnp.int32, (8, width), 0)
    lane8 = lax.broadcasted_iota(jnp.int32, (8, width), 1)
    masks = [
        (row8 // heads == i) & ((lane8 < half) == (lax.rem(row8, heads) == 0)) for i in range(2)
    ]
    place_columns = routing_places(group_ref[...] * EXPERTS_PER_GROUP + slot_ref[...])
    combine_table(place_columns, route_weight_ref[...], table_ref)
    table_copy = pltpu.make_async_copy(table_ref, table_hbm, w_sems.at[4])
    table_copy.start()
    tail = jnp.zeros((seqs, width), F32)
    for k, place in enumerate(place_columns):
        tail = tail + jnp.where(lane == k, place.astype(F32), 0.0)
    tail = tail.astype(BF16)
    for g in range(seqs // key_group):
        key_copies[g].wait()
        for s in range(g * key_group, (g + 1) * key_group, 2):
            masked = jnp.concatenate(
                [jnp.where(masks[i], query[s + i : s + i + 1], 0.0) for i in range(2)], axis=1
            ).astype(BF16)
            pair = jnp.concatenate([keys[s], keys[s + 1]], axis=1)
            result = lax.dot_general(masked, pair, NT, preferred_element_type=F32)
            for i in range(2):
                for h in range(heads):
                    scores[h * seqs + s + i : h * seqs + s + i + 1] = result[
                        heads * i + h : heads * i + h + 1
                    ]
    score = scores[...] * scale + (current - gate)
    score = jnp.where(entry < length, score, -jnp.inf)
    peak = jnp.maximum(jnp.max(score, axis=1, keepdims=True), own_score)
    weights = jnp.exp(score - peak)
    own_weight = jnp.exp(own_score - peak)
    denominator = jnp.sum(weights, axis=1, keepdims=True) + own_weight
    scores[...] = weights
    for g in range(seqs // value_group):
        value_copies[g].wait()
        for s in range(g * value_group, (g + 1) * value_group, 2):
            four = jnp.concatenate(
                [
                    scores[h * seqs + s + i : h * seqs + s + i + 1]
                    for i in range(2)
                    for h in range(heads)
                ]
                + [jnp.zeros((4, cache_len), F32)],
                axis=0,
            ).astype(BF16)
            pair = jnp.concatenate([values[s], values[s + 1]], axis=1)
            result = jnp.dot(four, pair, preferred_element_type=F32)
            for i in range(2):
                mine = result[heads * i : heads * i + heads, i * width : (i + 1) * width]
                weighted[s + i : s + i + 1] = jnp.where(first_head, mine[0:1], mine[1:2])
    output_copy.wait()
    table_copy.wait()
    own_weight = own_weight.astype(BF16).astype(F32)
    own_weight = jnp.where(first_head, own_weight[:seqs], own_weight[seqs:])
    denominator = jnp.where(first_head, denominator[:seqs], denominator[seqs:])
    attended = ((weighted[...] + own_weight * value_new) / denominator).astype(BF16)
    head_part = jnp.dot(attended, wo[...], preferred_element_type=F32).astype(BF16)
    model_width = head_part.shape[1]
    for i in range(parts_ref.shape[0]):
        parts_ref[i, :, 0:model_width] = head_part
        parts_ref[i, :, model_width:] = tail


def column_of(row):
    n = row.shape[1]
    same = lax.broadcasted_iota(jnp.int32, (n, n), 0) == lax.broadcasted_iota(
        jnp.int32, (n, n), 1
    )
    return jnp.sum(jnp.where(same, row.astype(F32), 0.0), axis=1, keepdims=True)


def routing_places(ids):
    picks, seqs = ids.shape
    columns = [column_of(ids[k : k + 1]) for k in range(picks)]
    down = lax.broadcasted_iota(jnp.int32, (seqs, seqs), 0)
    across = lax.broadcasted_iota(jnp.int32, (seqs, seqs), 1)
    rows = [ids[k : k + 1].astype(F32) for k in range(picks)]
    places = []
    for column in columns:
        before = jnp.zeros((seqs, 1), F32)
        for row in rows:
            hit = (column == row) & (across < down)
            before = before + jnp.sum(jnp.where(hit, 1.0, 0.0), axis=1, keepdims=True)
        places.append((column * 8 + before).astype(jnp.int32))
    return places


def select_table(place_rows, position, rows):
    seqs = place_rows[0].shape[1]
    row = lax.broadcasted_iota(jnp.int32, (rows, 4 * seqs), 0)
    column = lax.broadcasted_iota(jnp.int32, (rows, 4 * seqs), 1)
    expert = row >> 3
    is_dense = (row & 1) == 1
    token = column & (seqs - 1)
    hit = is_dense & (token == position * 2 + (expert & 1))
    for place in place_rows:
        places = jnp.concatenate([place] * 4, axis=1)
        hit = hit | (jnp.logical_not(is_dense) & (places == expert * 8 + (position & 1)))
    same_quarter = ((row >> 1) & 3) == column // seqs
    return jnp.where(hit & same_quarter, 1.0, 0.0).astype(BF16)


def combine_table(place_columns, weight_rows, table_ref):
    seqs = place_columns[0].shape[0]
    wide = table_ref.shape[1]
    row = lax.broadcasted_iota(jnp.int32, (2 * seqs, wide), 0)
    column = lax.broadcasted_iota(jnp.int32, (2 * seqs, wide), 1)
    is_dense = (column & 1) == 1
    core = (column >> 1) & 1
    chip = (column >> 3) & 3
    expert = column >> 5
    same_half = ((column >> 2) & 1) == (row >= seqs).astype(jnp.int32)
    weight = jnp.zeros((2 * seqs, wide), F32)
    for k, place in enumerate(place_columns):
        places = jnp.concatenate([place, place], axis=0)
        value = column_of(weight_rows[k : k + 1])
        value = jnp.concatenate([value, value], axis=0)
        hit = same_half & jnp.logical_not(is_dense) & (places == expert * 8 + core)
        weight = weight + jnp.where(hit, value, 0.0)
    high = weight.astype(BF16)
    table_ref[0 : 2 * seqs] = high
    table_ref[2 * seqs : 4 * seqs] = (weight - high.astype(F32)).astype(BF16)
    dense = same_half & is_dense & ((row & (seqs - 1)) == chip * 4 + core * 2 + (expert & 1))
    table_ref[4 * seqs : 6 * seqs] = jnp.where(dense, 1.0, 0.0).astype(BF16)


def dispatch_kernel(
    position_ref,
    parts_ref,
    tokens_ref,
    gain_ref,
    mix_ref,
    out_ref,
    residual_ref,
    mix_gate_ref,
    scratch,
):
    quarter = out_ref.shape[1]
    width = residual_ref.shape[1]
    model_width = tokens_ref.shape[1]
    seqs = tokens_ref.shape[0]
    columns = parts_ref[0, :, model_width:].astype(F32)
    same = lax.broadcasted_iota(jnp.int32, (seqs, seqs), 0) == lax.broadcasted_iota(
        jnp.int32, (seqs, seqs), 1
    )
    place_rows = [
        jnp.sum(jnp.where(same, columns[:, k : k + 1], 0.0), axis=0, keepdims=True).astype(
            jnp.int32
        )
        for k in range(2)
    ]
    select = select_table(place_rows, position_ref[0], out_ref.shape[0])
    attn = parts_ref[0, :, 0:model_width].astype(F32)
    for i in range(1, parts_ref.shape[0]):
        attn = attn + parts_ref[i, :, 0:model_width].astype(F32)
    residual = tokens_ref[...].astype(F32) + attn
    scratch[...] = residual
    normed = rms_scale(residual, gain_ref[...]).astype(BF16)
    quarters = jnp.concatenate(
        [normed[:, q * quarter : (q + 1) * quarter] for q in range(4)], axis=0
    )
    mix_gate_ref[...] = jax.nn.sigmoid(
        jnp.sum(normed.astype(F32) * mix_ref[...], axis=1, keepdims=True)
    )
    mine = pl.ds(pl.multiple_of(position_ref[0] * width, width), width)
    residual_ref[...] = scratch[:, mine]
    out_ref[...] = jnp.dot(select, quarters, preferred_element_type=F32).astype(BF16)


def whole_rows(parts):
    rows, width = parts.shape
    parts = parts.reshape(rows // 8, 8, width)
    parts = parts + pltpu.roll(parts, 4, 1)
    return (parts + pltpu.roll(parts, 2, 1)).reshape(rows, width)


def spread(values, out_ref, start):
    rows, quarter = values.shape
    values = values.astype(F32)
    row = lax.broadcasted_iota(jnp.int32, (rows, 1), 0)
    for q in range(4):
        mine = jnp.where(((row >> 1) & 3) == q, values, 0.0)
        out_ref[start : start + rows, q * quarter : (q + 1) * quarter] = mine.astype(BF16)


def picked_hidden(left, gate_ref, up_ref):
    width = gate_ref.shape[1]
    weights = jnp.concatenate([gate_ref[...], up_ref[...]], axis=1)
    both = whole_rows(jnp.dot(left, weights, preferred_element_type=F32))
    row = lax.broadcasted_iota(jnp.int32, (both.shape[0], 1), 0)
    hidden = silu(both[:, :width]) * both[:, width:]
    return jnp.where((row & 1) == 1, 0.0, hidden).astype(BF16)


def own_kernel(own_ref, gate_ref, up_ref, left_ref, picked_ref):
    spread(own_ref[...], left_ref, 0)
    picked_ref[...] = picked_hidden(left_ref[...], gate_ref, up_ref)


LATE = (1, 2, 3)


def split_pairs(operands):
    size = operands[0].shape[0] // 2
    return {
        2 * k + i: operands[k].at[pl.ds(i * size, size)]
        for k in sorted(range(len(operands)), key=LATE.count)
        for i in range(2)
    }


def down_block(position, k, hidden, down_ref, piece, rows):
    width = piece.shape[1]
    kb = 2 * width
    row = lax.broadcasted_iota(jnp.int32, (rows, 1), 0)
    right = ((row >> 2) & 1) == 1
    is_own = ((row >> 1) & 1) == (position & 1)
    dense_down = jnp.concatenate(
        [piece[2 * kb : 2 * kb + width], piece[2 * kb + width : 2 * kb + 2 * width]], axis=1
    )
    whole = pl.ds(pl.multiple_of((position ^ k) * kb, kb), kb)
    down = jnp.concatenate([down_ref[:, whole], dense_down], axis=0)
    result = jnp.dot(hidden, down, preferred_element_type=F32)
    result = jnp.where(is_own, result[:rows], result[rows:])
    result = jnp.where(right, result[:, width:], result[:, :width])
    return result.reshape(rows // 8, 8, width)


def expert_kernel(
    position_ref, left_ref, picked_ref, other_ref, gate_ref, up_ref, down_ref, *refs
):
    send_ref, hidden_ref, late, left, sems = refs[-5:]
    operands = list(refs[:-5])
    copies = [
        pltpu.make_async_copy(operands[k], late.at[i], sems.at[i]) for i, k in enumerate(LATE)
    ]
    for copy in copies:
        copy.start()
    for i, k in enumerate(LATE):
        operands[k] = late.at[i]
    pieces = split_pairs(operands)
    rows = other_ref.shape[0]
    width = late.shape[2]
    kb = 2 * width
    position = position_ref[0]
    spread(other_ref[...], left, 0)
    picked = picked_hidden(left[...], gate_ref, up_ref)
    sums = [None, None]
    for k, piece in pieces.items():
        if k == 2 * LATE[0]:
            for copy in copies:
                copy.wait()
        inner = pl.ds(pl.multiple_of((position ^ k) * kb, kb), kb)
        weights = jnp.concatenate([piece[0:kb], piece[kb : 2 * kb]], axis=1)
        for i, ref in enumerate((left_ref, left)):
            part = jnp.dot(ref[:, inner], weights, preferred_element_type=F32)
            sums[i] = part if sums[i] is None else sums[i] + part
    row = lax.broadcasted_iota(jnp.int32, (rows, 1), 0)
    for i, known in enumerate((picked_ref[...], picked)):
        both = whole_rows(sums[i])
        dense = silu(both[:, :width]) * both[:, width:]
        dense = jnp.where((row & 1) == 1, dense, 0.0).astype(BF16)
        hidden_ref[i * rows : (i + 1) * rows] = jnp.concatenate([known, dense], axis=1)
    hidden = hidden_ref[...]
    for k, piece in pieces.items():
        if k % 2 == 1:
            block = down_block(position, k, hidden, down_ref, piece, rows)
            send_ref[:, (position ^ k) >> 1] = block.astype(BF16)


def keep_kernel(position_ref, hidden_ref, down_ref, *refs):
    keep_ref = refs[-1]
    position = position_ref[0]
    hidden = hidden_ref[...]
    rows = hidden.shape[0] // 2
    for k, piece in split_pairs(refs[:-1]).items():
        if k % 2 == 0:
            block = down_block(position, k, hidden, down_ref, piece, rows)
            keep_ref[:, (position ^ k) >> 1] = block


def add_kernel(keep_ref, got_ref, out_ref):
    out_ref[...] = (keep_ref[...] + got_ref[...].astype(F32)).astype(BF16)


def combine_kernel(rows_ref, table_ref, mix_ref, residual_ref, out_ref):
    seqs = mix_ref.shape[0]
    width = rows_ref.shape[1]
    sums = jnp.dot(table_ref[...], rows_ref[...], preferred_element_type=F32)
    mix = mix_ref[...]
    for p in range(2):
        picked = sums[p * seqs : (p + 1) * seqs] + sums[(2 + p) * seqs : (3 + p) * seqs]
        dense = sums[(4 + p) * seqs : (5 + p) * seqs]
        columns = slice(p * width, (p + 1) * width)
        out_ref[:, columns] = (residual_ref[:, columns] + picked + mix * dense).astype(BF16)


def limits(mib):
    return pltpu.CompilerParams(vmem_limit_bytes=mib * MIB)


def exchange(array, axis):
    return lax.all_to_all(array, axis, 0, 0, tiled=True)


def attention_call(*operands):
    tokens, key_cache = operands[0], operands[13]
    seqs, model_width = tokens.shape
    _, cache_len, head_width = key_cache.shape
    tp_count = 8
    return pl.pallas_call(
        attention_kernel,
        name="attention",
        out_shape=(
            jax.ShapeDtypeStruct((tp_count, seqs, model_width + head_width), BF16),
            jax.ShapeDtypeStruct((6 * seqs, EXPERTS * 4 * tp_count), BF16),
        ),
        in_specs=[ANY] * 15,
        out_specs=(VMEM, ANY),
        scratch_shapes=[
            pltpu.VMEM((seqs, model_width), BF16),
            pltpu.VMEM((1, model_width), F32),
            pltpu.VMEM((2, model_width), BF16),
            pltpu.VMEM((1, 2), F32),
            pltpu.VMEM((seqs, 2, cache_len), F32),
            pltpu.VMEM((1, seqs), jnp.int32),
            pltpu.VMEM((1, seqs), jnp.int32),
            pltpu.VMEM((2, seqs), jnp.int32),
            pltpu.VMEM((2, seqs), F32),
            pltpu.VMEM((6 * seqs, EXPERTS * 4 * tp_count), BF16),
            pltpu.VMEM((3, model_width, head_width), BF16),
            pltpu.VMEM((head_width, model_width), BF16),
            pltpu.VMEM((seqs, cache_len, head_width), BF16),
            pltpu.VMEM((seqs, cache_len, head_width), BF16),
            pltpu.VMEM((2 * seqs, cache_len), F32),
            pltpu.VMEM((seqs, head_width), F32),
            pltpu.SemaphoreType.DMA((9,)),
            pltpu.SemaphoreType.DMA((5,)),
            pltpu.SemaphoreType.DMA((16,)),
            pltpu.SemaphoreType.DMA((16,)),
        ],
        compiler_params=limits(60),
        cost_estimate=pl.CostEstimate(flops=10**9, bytes_accessed=12 * MIB, transcendentals=40000),
    )(*operands)


def body(
    tokens,
    norm_attn,
    w_query,
    w_key,
    w_value,
    w_forget,
    forget_bias,
    w_output,
    key_cache,
    value_cache,
    gate_cache,
    lengths,
    norm_ffn,
    route_group,
    route_slot,
    route_weight,
    expert_gate,
    expert_up,
    expert_down,
    dense_gate,
    dense_up,
    dense_down,
    mix_vector,
):
    seqs, model_width = tokens.shape
    ep_count = lax.axis_size(EP)
    tp_count = lax.axis_size(TP)
    tp_position = lax.axis_index(TP)
    width_local = model_width // tp_count
    head_width = key_cache.shape[2]

    sibling = [(0, 1), (1, 0)]
    parts, table = attention_call(
        tokens,
        norm_attn.reshape(1, -1),
        w_forget.T,
        forget_bias.reshape(1, -1),
        gate_cache,
        lengths.reshape(1, -1),
        route_group.reshape(1, -1),
        route_slot.T,
        route_weight.T,
        w_query,
        w_key,
        w_value,
        w_output,
        key_cache,
        value_cache,
    )
    parts, dense_gate, dense_up, dense_down = lax.optimization_barrier(
        (parts, dense_gate, dense_up, dense_down)
    )
    own_dense = jnp.concatenate(
        [dense_gate, dense_up, dense_down[:, :head_width], dense_down[:, head_width:]], axis=0
    )
    ep_1 = lax.axis_size("ep_1")
    same, cross = [], []
    for e in range(ep_1):
        same += [(2 * e, 2 * e), (2 * e + 1, 2 * (e ^ 1) + 1)]
        cross += [(2 * e + 1, 2 * e), (2 * e, 2 * (e ^ 1) + 1)]
    first = []
    for route in (same, cross):
        first.append(lax.ppermute(own_dense, ("ep_1", "core"), route))
    pair = jnp.concatenate(first, axis=0)
    dense_weights = [pair]
    chips = lax.axis_size("y")
    for k in range(1, chips):
        dense_weights.append(lax.ppermute(pair, "y", [(i, i ^ k) for i in range(chips)]))
    parts = exchange(parts, TP)

    position = tp_position.reshape(1)
    row_count = ep_count * 8
    wide = row_count * tp_count // 2
    dispatch = pl.pallas_call(
        dispatch_kernel,
        name="dispatch",
        out_shape=(
            jax.ShapeDtypeStruct((row_count, model_width // 4), BF16),
            jax.ShapeDtypeStruct((seqs, width_local), F32),
            jax.ShapeDtypeStruct((seqs, 1), F32),
        ),
        in_specs=[SMEM] + [VMEM] * 4,
        out_specs=(VMEM, VMEM, VMEM),
        scratch_shapes=[pltpu.VMEM((seqs, model_width), F32)],
        compiler_params=limits(8),
    )
    outgoing, residual, mix_gate = dispatch(
        position,
        parts,
        tokens,
        norm_ffn.reshape(1, -1),
        mix_vector.reshape(1, -1),
    )
    arrived = exchange(outgoing.reshape(ep_count, 8, -1), EP).reshape(row_count, -1)
    other = lax.ppermute(arrived, "core", sibling)
    left, picked = pl.pallas_call(
        own_kernel,
        name="own",
        out_shape=(
            jax.ShapeDtypeStruct((row_count, model_width), BF16),
            jax.ShapeDtypeStruct((row_count, head_width), BF16),
        ),
        in_specs=[VMEM] * 3,
        out_specs=(VMEM, VMEM),
        compiler_params=limits(8),
    )(arrived, expert_gate[0], expert_up[0])
    blocks = (ep_count, tp_count // 2, 8, width_local // 2)
    send, hidden = pl.pallas_call(
        expert_kernel,
        name="experts",
        out_shape=(
            jax.ShapeDtypeStruct(blocks, BF16),
            jax.ShapeDtypeStruct((2 * row_count, 2 * head_width), BF16),
        ),
        in_specs=[SMEM] + [VMEM] * 6 + [ANY if k in LATE else VMEM for k in range(chips)],
        out_specs=(VMEM, VMEM),
        scratch_shapes=[
            pltpu.VMEM((len(LATE), *pair.shape), BF16),
            pltpu.VMEM((row_count, model_width), BF16),
            pltpu.SemaphoreType.DMA((len(LATE),)),
        ],
        compiler_params=limits(16),
    )(
        position,
        left,
        picked,
        other,
        expert_gate[0],
        expert_up[0],
        expert_down[0],
        *dense_weights,
    )
    got = lax.ppermute(send, "core", sibling)
    keep = pl.pallas_call(
        keep_kernel,
        name="keep",
        out_shape=jax.ShapeDtypeStruct(blocks, F32),
        in_specs=[SMEM] + [VMEM] * (2 + chips),
        out_specs=VMEM,
        compiler_params=limits(8),
    )(position, hidden, expert_down[0], *dense_weights)
    results = pl.pallas_call(
        add_kernel,
        name="add",
        out_shape=jax.ShapeDtypeStruct(blocks, BF16),
        in_specs=[VMEM] * 2,
        out_specs=VMEM,
        compiler_params=limits(8),
    )(keep, got)
    returned = exchange(
        results.reshape(ep_count * tp_count // 2, 8, width_local // 2), (*EP, "y")
    ).reshape(wide, width_local // 2)
    return pl.pallas_call(
        combine_kernel,
        name="combine",
        out_shape=jax.ShapeDtypeStruct((seqs, width_local), BF16),
        in_specs=[VMEM] * 4,
        out_specs=VMEM,
        compiler_params=limits(8),
    )(returned, table, mix_gate, residual)


def solution(mesh):
    split = Mesh(mesh.devices.reshape(8, 4, 4, 2), ("ep_0", "ep_1", "y", "core"))
    return jax.shard_map(
        body,
        mesh=split,
        in_specs=(
            P(EP, None),
            P(),
            P(None, TP),
            P(None, TP),
            P(None, TP),
            P(None, TP),
            P(TP),
            P(TP, None),
            P(EP, None, TP),
            P(EP, None, TP),
            P(EP, TP, None),
            P(EP),
            P(),
            P(EP),
            P(EP, None),
            P(EP, None),
            P(EP, None, TP),
            P(EP, None, TP),
            P(EP, TP, None),
            P(TP, EP),
            P(TP, EP),
            P(EP, TP),
            P(),
        ),
        out_specs=P(EP, TP),
        check_vma=False,
    )
```
